512 devices in a mesh: grp: 2 (over y), fs: 32 (over z), tp: 8 (over x, core).
Axes of the slice: x: 4, y: 2, z: 32, core: 2. Of those that a mesh axis runs over, the one named last changes fastest.
The devices are a block of a 4x8x32 slice.
Arguments:
- tokens: bfloat16 [64, 384, 2048], P(('grp', 'fs'), None, 'tp'), parts along dimension 0, may hold values from -24 to 24
- input_gain: float32 [2048], replicated, may hold values from 0.1 to 1.9
- query_weight: bfloat16 [2048, 1024], P('fs', 'tp'), may hold values from -0.125 to 0.125
- key_weight: bfloat16 [2048, 1024], P('fs', 'tp'), may hold values from -0.125 to 0.125
- value_weight: bfloat16 [2048, 1024], P('fs', 'tp'), may hold values from -0.125 to 0.125
- output_gate_matrix: bfloat16 [2048, 1024], P('fs', 'tp'), may hold values from -0.125 to 0.125
- forward_decay: float32 [16], P('tp'), may hold values from -1 to 9
- backward_decay: float32 [16], P('tp'), may hold values from -1 to 9
- merge_weight: bfloat16 [1024, 2048], P('tp', 'fs'), may hold values from -0.375 to 0.375
- middle_gain: float32 [2048], replicated, may hold values from 0.1 to 1.9
- gate_weight: bfloat16 [2048, 5120], P('fs', 'tp'), may hold values from -0.125 to 0.125
- up_weight: bfloat16 [2048, 5120], P('fs', 'tp'), may hold values from -0.125 to 0.125
- down_weight: bfloat16 [5120, 2048], P('tp', 'fs'), may hold values from -0.15625 to 0.15625
Outputs:
- layer_out: bfloat16 [64, 384, 2048], P(('grp', 'fs'), None, 'tp'), parts along dimension 0
The draws below stay inside these ranges and needn't reach their ends.
There are 2 independent parts, one for each index of `grp`. The reference program is written for one: setup_inputs(seed, part) draws one part's arguments, and reference() takes and returns one part's arrays. A program takes and returns all parts, laid end to end along the dimension named above; an argument that names none is the same for every part. Nothing has to cross between parts.
All inputs are finite; a program needn't handle non-finite values.
Results may differ from the reference program's by a relative error of at most 0.019.
Values may be sent and summed in bfloat16 or wider, within the bound.
A program may use at most 64 MiB of HBM per device.

```python
import math
import jax
import jax.numpy as jnp
from jax import lax

D = 2048
HEADS = 16
FF = 5120
BLOCK = 128
LEN = 384
RET_W = 1024
SEQS = 32
N_TP = 8


def draw_tokens(key, part):
    subkeys = jax.random.split(jax.random.fold_in(key, 11), 3)
    full_shape = (SEQS, LEN, D)
    row_scale = jnp.exp(jax.random.uniform(subkeys[1], (SEQS, LEN, 1), jnp.float32, math.log(0.3), math.log(3.0)))
    column_scale = jnp.exp(jax.random.uniform(subkeys[2], (1, 1, D), jnp.float32, math.log(0.5), math.log(2.0)))
    base_values = jnp.clip(jax.random.normal(subkeys[0], full_shape, jnp.float32), -4.0, 4.0)
    return (base_values * row_scale * column_scale).astype(jnp.bfloat16)


def decay_logits(key, salt):
    subkeys = jax.random.split(jax.random.fold_in(key, salt), 3)
    slow_share = 0.5
    slow_low = 0.7
    slow_high = 2.3
    is_slow = jax.random.bernoulli(subkeys[0], slow_share, (HEADS,))
    slow_rate = -jax.random.uniform(subkeys[1], (HEADS,), jnp.float32, slow_low, slow_high) / LEN
    fast_rate = -jax.random.uniform(subkeys[2], (HEADS,), jnp.float32, 7.5, 15.0) / BLOCK
    log_rates = jnp.where(is_slow, slow_rate, fast_rate)
    return log_rates - jnp.log(-jnp.expm1(log_rates))


def draw_forward_decay(key, part):
    return decay_logits(key, 21)


def draw_backward_decay(key, part):
    return decay_logits(key, 22)


def levels(stream_key, dims, pieces, smallest, largest):
    gain, own = 1.0, jax.random.fold_in(stream_key, 6)
    for dim, blocks in pieces:
        draws = jnp.exp(jax.random.uniform(jax.random.fold_in(own, dim), (blocks,), jnp.float32, smallest / len(pieces), largest / len(pieces)))
        gain = gain * jnp.repeat(draws, dims[dim] // blocks).reshape([-1 if axis == dim else 1 for axis in range(len(dims))])
    return gain


def scatter_about(stream_key, shape, scale, bound, cuts=(), kind=jnp.bfloat16):
    level = levels(stream_key, shape, cuts, -0.22, 0.18) if cuts else 1.0
    values = jax.random.normal(stream_key, shape, jnp.float32) * scale * level
    return jnp.minimum(jnp.maximum(values, -bound), bound).astype(kind)


def setup_inputs(seed: int = 0, part: int = 0) -> dict:
    arg_keys = jax.random.split(jax.random.key(seed), 14)
    part_splits = jax.random.split(jax.random.fold_in(arg_keys[13], part), 14)
    return {
        "tokens": draw_tokens(jax.random.fold_in(jax.random.fold_in(arg_keys[13], part), 71), part),
        "input_gain": jnp.clip(1.0 + 0.18 * jax.random.normal(arg_keys[1], (D,), jnp.float32), 0.1, 1.9),
        "query_weight": scatter_about(arg_keys[2], (D, RET_W), D ** -0.5, 0.125, ((0, 32), (1, 8))),
        "key_weight": scatter_about(arg_keys[3], (D, RET_W), D ** -0.5, 0.125, ((0, 32), (1, 8))),
        "value_weight": scatter_about(arg_keys[4], (D, RET_W), D ** -0.5, 0.125, ((0, 32), (1, 8))),
        "output_gate_matrix": scatter_about(arg_keys[5], (D, RET_W), D ** -0.5, 0.125, ((0, 32), (1, 8))),
        "forward_decay": draw_forward_decay(jax.random.fold_in(arg_keys[13], 71), part),
        "backward_decay": draw_backward_decay(jax.random.fold_in(arg_keys[13], 71), part),
        "merge_weight": scatter_about(arg_keys[8], (RET_W, D), (RET_W // 4) ** -0.5, 0.375, ((0, 8), (1, 32))),
        "middle_gain": jnp.clip(1.0 + 0.18 * jax.random.normal(arg_keys[9], (D,), jnp.float32), 0.1, 1.9),
        "gate_weight": scatter_about(arg_keys[10], (D, FF), D ** -0.5, 0.125, ((0, 32), (1, 8))),
        "up_weight": scatter_about(arg_keys[11], (D, FF), D ** -0.5, 0.125, ((0, 32), (1, 8))),
        "down_weight": scatter_about(arg_keys[12], (FF, D), (FF // 4) ** -0.5, 0.15625, ((0, 8), (1, 32))),
    }


norm_eps = 1e-06
group_eps = 1e-05
rope_base = 10000.0
highest_precision = lax.Precision.HIGHEST

def rms_scale(values, gain_vector):
    widened = values.astype(jnp.float32)
    scaled = widened * lax.rsqrt(lax.optimization_barrier(jnp.mean(widened * widened, axis=-1, keepdims=True)) + norm_eps)
    return (scaled * gain_vector.astype(jnp.float32)).astype(jnp.bfloat16)

def apply_rotary_heads(values, length):
    half_dim = values.shape[-1] // 2
    inverse = rope_base ** (-jnp.arange(half_dim, dtype=jnp.float32) / half_dim)
    angles = jnp.arange(length, dtype=jnp.float32)[:, None] * inverse[None, :]
    cosine = jnp.cos(angles)[:, None, :]
    sine_part = jnp.sin(angles)[:, None, :]
    lower_half = values[..., :half_dim]
    upper_half = values[..., half_dim:]
    return jnp.concatenate([lower_half * cosine - upper_half * sine_part, upper_half * cosine + lower_half * sine_part], axis=-1)

def retain_dense(query_rows, key_rows, value_rows, gate_rows, forward_decay, backward_decay, seq_count, length):
    head_count = forward_decay.shape[0]
    head_dim = query_rows.shape[1] // head_count

    def split_heads(rows_in):
        return rows_in.astype(jnp.float32).reshape(seq_count, length, head_count, head_dim)
    queries = apply_rotary_heads(split_heads(query_rows), length)
    key_heads = apply_rotary_heads(split_heads(key_rows), length) * head_dim ** (-0.5)
    valued = split_heads(value_rows)
    rate_ahead = jax.nn.log_sigmoid(forward_decay.astype(jnp.float32))
    rate_behind = jax.nn.log_sigmoid(backward_decay.astype(jnp.float32))
    position = jnp.arange(length, dtype=jnp.float32)
    offset = position[:, None] - position[None, :]
    weight_tree = jnp.where(offset[None] >= 0, jnp.exp(rate_ahead[:, None, None] * jnp.maximum(offset, 0.0)[None]), jnp.exp(rate_behind[:, None, None] * jnp.maximum(-offset, 0.0)[None]))

    def one_sequence(operands):
        sequence_query, sequence_key, sequence_value = operands
        attention_scores = jnp.einsum('pze,rze->zpr', sequence_query, sequence_key, precision=highest_precision) * weight_tree
        return jnp.einsum('kaf,fkg->akg', attention_scores, sequence_value, precision=highest_precision)
    result = lax.map(one_sequence, (queries, key_heads, valued))
    center = lax.optimization_barrier(jnp.mean(result, axis=-1, keepdims=True))
    spread = lax.optimization_barrier(jnp.mean(jnp.square(result - center), axis=-1, keepdims=True))
    normalized = (result - center) * lax.rsqrt(spread + group_eps)
    gated = jax.nn.silu(split_heads(gate_rows)) * normalized
    return gated.reshape(seq_count * length, head_count * head_dim).astype(jnp.bfloat16)

def split_sum(left_rows, right_rows):
    group_size = left_rows.shape[1] // N_TP
    total = jnp.zeros((left_rows.shape[0], right_rows.shape[1]), jnp.float32)
    for index in range(N_TP):
        lower = index * group_size
        partial_term = jnp.dot(left_rows[:, lower:lower + group_size], right_rows[lower:lower + group_size], preferred_element_type=jnp.float32).astype(jnp.bfloat16)
        total = total + lax.optimization_barrier(partial_term).astype(jnp.float32)
    return total

def reference(tokens, input_gain, query_weight, key_weight, value_weight, output_gate_matrix, forward_decay, backward_decay, merge_weight, middle_gain, gate_weight, up_weight, down_weight):
    seq_count, length, width = tokens.shape
    row_count = seq_count * length
    flat = tokens.reshape(row_count, width)
    normed = rms_scale(flat, input_gain)
    query_rows = jnp.dot(normed, query_weight, preferred_element_type=jnp.float32).astype(jnp.bfloat16)
    key_rows = jnp.dot(normed, key_weight, preferred_element_type=jnp.float32).astype(jnp.bfloat16)
    value_rows = jnp.dot(normed, value_weight, preferred_element_type=jnp.float32).astype(jnp.bfloat16)
    gate_rows = jnp.dot(normed, output_gate_matrix, preferred_element_type=jnp.float32).astype(jnp.bfloat16)
    mixed = retain_dense(query_rows, key_rows, value_rows, gate_rows, forward_decay, backward_decay, seq_count, length)
    middle = (flat.astype(jnp.float32) + split_sum(mixed, merge_weight)).astype(jnp.bfloat16)
    normed_mid = rms_scale(middle, middle_gain)
    gate_act = jnp.dot(normed_mid, gate_weight, preferred_element_type=jnp.float32)
    up_act = jnp.dot(normed_mid, up_weight, preferred_element_type=jnp.float32)
    hidden = (jax.nn.silu(gate_act) * up_act).astype(jnp.bfloat16)
    layer_out = (middle.astype(jnp.float32) + split_sum(hidden, down_weight)).astype(jnp.bfloat16)
    return layer_out.reshape(seq_count, length, width)
```

```python
import functools

import jax
import jax.numpy as jnp
import numpy as np
from jax import lax
from jax.experimental import pallas as pl
from jax.experimental.pallas import tpu as pltpu
from jax.sharding import PartitionSpec as P

MESH = pl.DeviceIdType.MESH
HEAD = 64
NORM_EPS = 1e-06
GROUP_EPS = 1e-05
ROPE_BASE = 10000.0
F32 = jnp.float32
BF16 = jnp.bfloat16

NT_DIMS = (((1,), (1,)), ((), ()))


def rotation_tables(length):
    half = HEAD // 2
    inverse = ROPE_BASE ** (-np.arange(half, dtype=np.float32) / np.float32(half))
    angles = np.arange(length, dtype=np.float32)[:, None] * inverse.astype(np.float32)[None, :]
    cosine, sine = np.cos(angles), np.sin(angles)
    return (
        np.concatenate([cosine, cosine] * 2, axis=1).astype(np.float32),
        np.concatenate([-sine, sine] * 2, axis=1).astype(np.float32),
    )


def remote(src, dst, send_sem, recv_sem, device):
    return pltpu.make_async_remote_copy(
        src_ref=src, dst_ref=dst, send_sem=send_sem, recv_sem=recv_sem, device_id=device, device_id_type=MESH
    )


def layer_kernel(
    nf,
    nt,
    tok,
    gain1,
    wq,
    wk,
    wv,
    wo,
    fdec,
    bdec,
    wm,
    gain2,
    wgate,
    wup,
    wdown,
    cos,
    sin,
    out,
    a_buf,
    m_buf,
    g_buf,
    d_buf,
    m_stage,
    d_stage,
    tok_all,
    nrm,
    decay,
    qkvg,
    mixed,
    part,
    part_in,
    mid_all,
    hid,
    fin_out,
    fin_in,
    local_sem,
    ring_send,
    ring_recv,
    tok_send,
    tok_recv,
    part_send,
    part_recv,
    mid_send,
    mid_recv,
    fin_send,
    fin_recv,
):
    z = lax.axis_index("fs")
    t = lax.axis_index("tp")
    right, left = lax.rem(z + 1, nf), lax.rem(z + nf - 1, nf)
    far = nf // 2
    rows = tok.shape[0]
    width = tok.shape[1]
    per = wq.shape[0]
    cols = wq.shape[1]
    ff = wgate.shape[1]
    per_tp = width // per

    base = pl.multiple_of(z * per, per)
    mine = pl.ds(base, per)
    copies = [pltpu.make_async_copy(tok, tok_all.at[t], local_sem.at[0])]
    for n, w in enumerate((wq, wk, wv, wo)):
        copies.append(pltpu.make_async_copy(w, a_buf.at[mine, pl.ds(n * cols, cols)], local_sem.at[1 + n]))
    copies.append(pltpu.make_async_copy(wm, m_stage, local_sem.at[5]))
    copies.append(pltpu.make_async_copy(wgate, g_buf.at[mine, pl.ds(0, ff)], local_sem.at[6]))
    copies.append(pltpu.make_async_copy(wup, g_buf.at[mine, pl.ds(ff, ff)], local_sem.at[7]))
    copies.append(pltpu.make_async_copy(wdown, d_stage, local_sem.at[8]))
    for c in copies:
        c.start()

    barrier = pltpu.get_barrier_semaphore()
    for side in (left, right):
        pl.semaphore_signal(barrier, inc=1, device_id={"fs": side}, device_id_type=MESH)
    for k in range(1, nt):
        pl.semaphore_signal(barrier, inc=1, device_id={"tp": lax.rem(t + k, nt)}, device_id_type=MESH)
    pl.semaphore_wait(barrier, nt + 1)

    def hop(cls, s, wait_r, wait_l, send_r, send_l):
        buf, off, size, i = cls
        from_left = buf.at[pl.ds(pl.multiple_of(lax.rem(z - s + nf, nf) * per + off, 16), size)]
        from_right = buf.at[pl.ds(pl.multiple_of(lax.rem(z + s, nf) * per + off, 16), size)]
        if wait_r:
            remote(from_left, from_left, ring_send.at[i], ring_recv.at[i, 0, s], {"fs": left}).wait_recv()
        if send_r:
            remote(from_left, from_left, ring_send.at[i], ring_recv.at[i, 0, s + 1], {"fs": right}).start()
        if wait_l:
            remote(from_right, from_right, ring_send.at[i], ring_recv.at[i, 1, s], {"fs": right}).wait_recv()
        if send_l:
            remote(from_right, from_right, ring_send.at[i], ring_recv.at[i, 1, s + 1], {"fs": left}).start()

    def rounds(classes, lo, hi):
        if lo == 0 and hi > 0:
            for c in classes:
                hop(c, 0, False, False, True, True)
            lo = 1
        stop = min(hi, far - 1)
        if stop > lo:

            def body(s, carry):
                for c in classes:
                    hop(c, s, True, True, True, True)
                return carry

            lax.fori_loop(lo, stop, body, 0)
        if lo <= far - 1 < hi:
            for c in classes:
                hop(c, far - 1, True, True, True, False)
        if lo <= far < hi:
            for c in classes:
                hop(c, far, True, False, False, False)

    first = [(a_buf, 0, 32, 0), (a_buf, 32, 32, 1), (m_buf, 0, 64, 2), (g_buf, 0, 16, 3)]
    second = [(g_buf, 16, 16, 4), (g_buf, 32, 16, 5), (g_buf, 48, 16, 6)]
    third = [(d_buf, 0, 32, 7), (d_buf, 32, 32, 8)]

    def spread(buf, send_sem, recv_sem):
        def body(k, carry):
            j = lax.rem(t + k, nt)
            remote(buf.at[t], buf.at[t], send_sem.at[0], recv_sem.at[t], {"tp": j}).start()
            return carry

        lax.fori_loop(1, nt, body, 0)

    def arrived(buf, send_sem, recv_sem):
        def body(k, carry):
            j = lax.rem(t + k, nt)
            remote(buf.at[j], buf.at[j], send_sem.at[0], recv_sem.at[j], {"tp": j}).wait_recv()
            return carry

        lax.fori_loop(1, nt, body, 0)

    def normalize(src, gain):
        total = jnp.zeros((rows, 1), F32)
        for j in range(nt):
            v = src[j].astype(F32)
            total = total + jnp.sum(v * v, axis=-1, keepdims=True)
        scale = lax.rsqrt(total * (1.0 / (nt * width)) + NORM_EPS)
        for j in range(nt):
            span = pl.ds(j * width, width)
            nrm[:, span] = (src[j].astype(F32) * scale * gain[:, span]).astype(BF16)

    copies[0].wait()
    spread(tok_all, tok_send, tok_recv)
    for c in copies[1:5]:
        c.wait()
    rounds(first[:2], 0, 1)
    copies[5].wait()
    m_buf[mine, :] = m_stage[...].astype(F32).T.astype(BF16)
    copies[6].wait()
    copies[7].wait()
    rounds(first[3:], 0, 1)
    rounds(first[2:3], 0, 1)

    n_id = lax.broadcasted_iota(jnp.int32, (128, rows), 0)
    m_id = lax.broadcasted_iota(jnp.int32, (128, rows), 1)
    lane = lax.broadcasted_iota(jnp.int32, (rows, 2 * HEAD), 1)
    low_head = lane < HEAD
    fwd = jax.nn.log_sigmoid(fdec[...])
    bwd = jax.nn.log_sigmoid(bdec[...])
    for h in range(2):
        for c in range(rows // 128):
            gap = (n_id + (c * 128) - m_id).astype(F32)
            exponent = jnp.where(gap >= 0, fwd[:, h : h + 1] * gap, bwd[:, h : h + 1] * (-gap))
            decay[h, pl.ds(c * 128, 128), :] = jnp.exp(exponent)
        rounds(first, 1 + h, 2 + h)
    copies[8].wait()
    d_buf[mine, :] = d_stage[...].astype(F32).T.astype(BF16)
    rounds(first, 3, 7)
    arrived(tok_all, tok_send, tok_recv)
    normalize(tok_all, gain1)
    rounds(first, 7, far)
    rounds(second, 0, 1)
    rounds(first, far, far + 1)

    for n in range(4):
        span = pl.ds(n * cols, cols)
        qkvg[:, span] = jnp.dot(nrm[...], a_buf[:, span], preferred_element_type=F32).astype(BF16)
    rounds(second, 1, 2)

    def rotated(n):
        v = qkvg[:, pl.ds(n * cols, cols)].astype(F32)
        lo_half = lax.rem(lane, HEAD) < HEAD // 2
        swapped = jnp.where(lo_half, pltpu.roll(v, 2 * HEAD - HEAD // 2, 1), pltpu.roll(v, HEAD // 2, 1))
        return v * cos[...] + swapped * sin[...]

    rq = rotated(0)
    rk = (rotated(1) * HEAD**-0.5).astype(BF16)
    value = qkvg[:, pl.ds(2 * cols, cols)]
    rounds(second, 2, 3)
    kept = []
    for h in range(2):
        q_h = jnp.where(low_head if h == 0 else jnp.logical_not(low_head), rq, 0.0).astype(BF16)
        parts = []
        for c in range(rows // 128):
            scores = lax.dot_general(q_h[c * 128 : (c + 1) * 128], rk, NT_DIMS, preferred_element_type=F32)
            weighted = (scores * decay[h, pl.ds(c * 128, 128), :]).astype(BF16)
            parts.append(jnp.dot(weighted, value, preferred_element_type=F32))
        kept.append(jnp.concatenate(parts, axis=0))
        rounds(second, 3 + h, 4 + h)
    retained = jnp.where(low_head, kept[0], kept[1])

    def head_mean(v):
        lo = jnp.sum(jnp.where(low_head, v, 0.0), axis=-1, keepdims=True)
        hi = jnp.sum(jnp.where(low_head, 0.0, v), axis=-1, keepdims=True)
        return jnp.where(low_head, lo, hi) * (1.0 / HEAD)

    centered = retained - head_mean(retained)
    normalized = centered * lax.rsqrt(head_mean(centered * centered) + GROUP_EPS)
    gate = qkvg[:, pl.ds(3 * cols, cols)].astype(F32)
    mixed[...] = (gate / (1.0 + jnp.exp(-gate)) * normalized).astype(BF16)

    def project(k, carry):
        j = lax.rem(t + k, nt)
        w = m_buf[pl.ds(pl.multiple_of(j * width, width), width), :]
        part[j] = lax.dot_general(mixed[...], w, NT_DIMS, preferred_element_type=F32).astype(BF16)

        @pl.when(k < nt)
        def _():
            remote(part.at[j], part_in.at[t], part_send.at[0], part_recv.at[t], {"tp": j}).start()

        return carry

    lax.fori_loop(1, nt + 1, project, 0)
    rounds(second, 5, 11)

    def part_wait(k, carry):
        j = lax.rem(t + k, nt)
        remote(part.at[j], part_in.at[j], part_send.at[0], part_recv.at[j], {"tp": j}).wait_recv()
        return carry

    lax.fori_loop(1, nt, part_wait, 0)
    total = tok_all[t].astype(F32) + part[t].astype(F32)
    for k in range(1, nt):
        total = total + part_in[lax.rem(t + k, nt)].astype(F32)
    mid_all[t] = total.astype(BF16)
    rounds(second, 11, 12)
    spread(mid_all, mid_send, mid_recv)
    rounds(second, 12, far)
    rounds(third, 0, 1)
    rounds(second, far, far + 1)
    rounds(third, 1, 3)
    arrived(mid_all, mid_send, mid_recv)
    normalize(mid_all, gain2)
    at = 3
    for c in range(ff // 128):
        g = jnp.dot(nrm[...], g_buf[:, pl.ds(c * 128, 128)], preferred_element_type=F32)
        u = jnp.dot(nrm[...], g_buf[:, pl.ds(ff + c * 128, 128)], preferred_element_type=F32)
        hid[:, pl.ds(c * 128, 128)] = (g / (1.0 + jnp.exp(-g)) * u).astype(BF16)
        rounds(third, at, at + 1)
        at += 1

    def block(b):
        w = d_buf[pl.ds(pl.multiple_of(b * per, per), per), :]
        fin_out[b] = lax.dot_general(w, hid[...], NT_DIMS, preferred_element_type=F32).astype(BF16)
        j = lax.div(b, per_tp)
        q = b - j * per_tp

        @pl.when(j == t)
        def _():
            fin_in[t, q] = fin_out[b]

        @pl.when(j != t)
        def _():
            remote(fin_out.at[b], fin_in.at[t, q], fin_send.at[0], fin_recv.at[t, q], {"tp": j}).start()

    def pair(d):
        block(lax.rem(z - d + nf, nf))
        block(lax.rem(z + d, nf))

    block(z)
    done = 1
    span = far - at

    def catch_up(i, carry):
        for c in third:
            hop(c, at + i, True, True, True, True)
        pair(2 * i + 1)
        pair(2 * i + 2)
        return carry

    steps = far - 1 - at
    lax.fori_loop(0, steps, catch_up, 0)
    done = 2 * steps + 1
    rounds(third, far - 1, far)

    def rest(d, carry):
        pair(d)
        return carry

    lax.fori_loop(done, far, rest, 0)
    rounds(third, far, far + 1)
    block(lax.rem(z + far, nf))

    def fin_wait(k, carry):
        j = lax.rem(t + k, nt)
        for q in range(per_tp):
            remote(fin_out.at[0], fin_in.at[j, q], fin_send.at[0], fin_recv.at[j, q], {"tp": j}).wait_recv()
        return carry

    lax.fori_loop(1, nt, fin_wait, 0)
    for q in range(per_tp):
        total = fin_in[0, q].astype(F32)
        for j in range(1, nt):
            total = total + fin_in[j, q].astype(F32)
        fin_sum = total.T
        span_q = pl.ds(q * per, per)
        out[:, span_q] = (mid_all[t, :, span_q].astype(F32) + fin_sum).astype(BF16)

    for buf, off, size, i in first + second + third:
        whole = buf.at[pl.ds(0, (nf - 1) * size)]
        remote(whole, whole, ring_send.at[i], ring_recv.at[i, 0, 0], {"fs": right}).wait_send()
    for buf, sem in ((tok_all, tok_send), (part, part_send), (mid_all, mid_send)):
        whole = buf.at[pl.ds(0, nt - 1)]
        remote(whole, whole, sem.at[0], tok_recv.at[0], {"tp": lax.rem(t + 1, nt)}).wait_send()
    whole = fin_out.at[pl.ds(0, nf - per_tp)]
    remote(whole, whole, fin_send.at[0], fin_recv.at[0, 0], {"tp": lax.rem(t + 1, nt)}).wait_send()


def on_device(nf, nt, tokens, input_gain, wq, wk, wv, wo, fdec, bdec, wm, middle_gain, wgate, wup, wdown):
    seqs, rows, width = tokens.shape
    per, cols = wq.shape
    ff = wgate.shape[1]
    full = nf * per
    cos, sin = rotation_tables(rows)
    anywhere = pl.BlockSpec(memory_space=pl.ANY)
    vmem = pl.BlockSpec(memory_space=pltpu.VMEM)
    dma = pltpu.SemaphoreType.DMA
    out = pl.pallas_call(
        functools.partial(layer_kernel, nf, nt),
        out_shape=jax.ShapeDtypeStruct((rows, width), BF16),
        in_specs=[
            anywhere,
            vmem,
            anywhere,
            anywhere,
            anywhere,
            anywhere,
            vmem,
            vmem,
            anywhere,
            vmem,
            anywhere,
            anywhere,
            anywhere,
            vmem,
            vmem,
        ],
        out_specs=vmem,
        scratch_shapes=[
            pltpu.VMEM((full, 4 * cols), BF16),
            pltpu.VMEM((full, wm.shape[0]), BF16),
            pltpu.VMEM((full, 2 * ff), BF16),
            pltpu.VMEM((full, ff), BF16),
            pltpu.VMEM(wm.shape, BF16),
            pltpu.VMEM(wdown.shape, BF16),
            pltpu.VMEM((nt, rows, width), BF16),
            pltpu.VMEM((rows, full), BF16),
            pltpu.VMEM((2, rows, rows), F32),
            pltpu.VMEM((rows, 4 * cols), BF16),
            pltpu.VMEM((rows, cols), BF16),
            pltpu.VMEM((nt, rows, width), BF16),
            pltpu.VMEM((nt, rows, width), BF16),
            pltpu.VMEM((nt, rows, width), BF16),
            pltpu.VMEM((rows, ff), BF16),
            pltpu.VMEM((nf, per, rows), BF16),
            pltpu.VMEM((nt, width // per, per, rows), BF16),
            dma((9,)),
            dma((9,)),
            dma((9, 2, nf // 2 + 1)),
            dma((1,)),
            dma((nt,)),
            dma((1,)),
            dma((nt,)),
            dma((1,)),
            dma((nt,)),
            dma((1,)),
            dma((nt, width // per)),
        ],
        compiler_params=pltpu.CompilerParams(
            collective_id=0, has_side_effects=True, vmem_limit_bytes=60 * 1024 * 1024
        ),
    )(
        tokens.reshape(seqs * rows, width),
        input_gain.reshape(1, -1),
        wq,
        wk,
        wv,
        wo,
        fdec.reshape(1, -1),
        bdec.reshape(1, -1),
        wm,
        middle_gain.reshape(1, -1),
        wgate,
        wup,
        wdown,
        jnp.asarray(cos),
        jnp.asarray(sin),
    )
    return out.reshape(seqs, rows, width)


def solution(mesh):
    sizes = dict(mesh.shape)
    placed = (
        P(("grp", "fs"), None, "tp"),
        P(),
        P("fs", "tp"),
        P("fs", "tp"),
        P("fs", "tp"),
        P("fs", "tp"),
        P("tp"),
        P("tp"),
        P("tp", "fs"),
        P(),
        P("fs", "tp"),
        P("fs", "tp"),
        P("tp", "fs"),
    )
    return jax.shard_map(
        functools.partial(on_device, sizes["fs"], sizes["tp"]),
        mesh=mesh,
        in_specs=placed,
        out_specs=P(("grp", "fs"), None, "tp"),
        check_vma=False,
    )
```

```python
import functools

import jax
import jax.numpy as jnp
import numpy as np
from jax import lax
from jax.experimental import pallas as pl
from jax.experimental.pallas import tpu as pltpu
from jax.sharding import PartitionSpec as P

MESH = pl.DeviceIdType.MESH
HEAD = 64
NORM_EPS = 1e-06
GROUP_EPS = 1e-05
ROPE_BASE = 10000.0
F32 = jnp.float32
BF16 = jnp.bfloat16

D_START = 12

NT_DIMS = (((1,), (1,)), ((), ()))


def rotation_tables(length):
    half = HEAD // 2
    inverse = ROPE_BASE ** (-np.arange(half, dtype=np.float32) / np.float32(half))
    angles = np.arange(length, dtype=np.float32)[:, None] * inverse.astype(np.float32)[None, :]
    cosine, sine = np.cos(angles), np.sin(angles)
    return (
        np.concatenate([cosine, cosine] * 2, axis=1).astype(np.float32),
        np.concatenate([-sine, sine] * 2, axis=1).astype(np.float32),
    )


def remote(src, dst, send_sem, recv_sem, device):
    return pltpu.make_async_remote_copy(
        src_ref=src, dst_ref=dst, send_sem=send_sem, recv_sem=recv_sem, device_id=device, device_id_type=MESH
    )


def layer_kernel(
    nf,
    nt,
    tok,
    gain1,
    wq,
    wk,
    wv,
    wo,
    fdec,
    bdec,
    wm,
    gain2,
    wgate,
    wup,
    wdown,
    cos,
    sin,
    out,
    a_buf,
    g_buf,
    d_buf,
    tok_all,
    mid_all,
    nrm,
    decay,
    qacc,
    qkvg,
    mixed,
    acts,
    hid,
    own,
    ship1,
    got1,
    sums1,
    over1,
    last1,
    ship2,
    got2,
    sums2,
    over2,
    last2,
    local_sem,
    ring_send,
    ring_recv,
    pair_send,
    pair_recv,
    tok_send,
    tok_recv,
    mid_send,
    mid_recv,
    rs1_send,
    rs1_recv,
    rs2_send,
    rs2_recv,
):
    g = lax.axis_index("grp")
    z = lax.axis_index("fs")
    t = lax.axis_index("tp")
    nx = nt // 2
    x, c = lax.div(t, 2), lax.rem(t, 2)
    parity = lax.rem(g, 2)
    twin = {"grp": g + 1 - 2 * parity}
    right, left = {"fs": lax.rem(z + 1, nf)}, {"fs": lax.rem(z + nf - 1, nf)}

    def tp_of(dx, core):
        return lax.rem(x + dx + nx, nx) * 2 + core

    xr, xl, other = {"tp": tp_of(1, c)}, {"tp": tp_of(-1, c)}, {"tp": tp_of(0, 1 - c)}
    far = nf // 2
    rows, width = tok.shape
    half = rows // 2
    per, cols = wq.shape
    ff = wgate.shape[1]
    mcol = 4 * cols
    tiles = width // per

    mine = pl.ds(pl.multiple_of(z * per, per), per)
    copies = [pltpu.make_async_copy(tok, tok_all.at[t], local_sem.at[0])]
    for n, w in enumerate((wq, wk, wv, wo, wm)):
        copies.append(pltpu.make_async_copy(w, a_buf.at[mine, pl.ds(n * cols, cols)], local_sem.at[1 + n]))
    copies.append(pltpu.make_async_copy(wgate, g_buf.at[mine, pl.ds(0, ff)], local_sem.at[6]))
    copies.append(pltpu.make_async_copy(wup, g_buf.at[mine, pl.ds(ff, ff)], local_sem.at[7]))
    copies.append(pltpu.make_async_copy(wdown, d_buf.at[mine, :], local_sem.at[8]))
    for copy in copies:
        copy.start()

    barrier = pltpu.get_barrier_semaphore()
    for peer in (left, right, xl, xr, other, twin):
        pl.semaphore_signal(barrier, inc=1, device_id=peer, device_id_type=MESH)
    pl.semaphore_wait(barrier, 6)

    def shared(buf, row0, nrow, col0, ncol, by_row, i, k):
        step_r, step_c = (nrow, 0) if by_row else (0, ncol)
        flip = 1 - parity
        return (buf, row0 + step_r * parity, nrow, col0 + step_c * parity, ncol, i, k, row0 + step_r * flip, col0 + step_c * flip)

    g_common, g_half = 4 * 128, 3 * 128
    d_common, d_half = 128, 2 * 128
    cls_a = shared(a_buf, 0, per // 2, 0, mcol + wm.shape[1], True, 0, 0)
    cls_g0 = (g_buf, 0, per, 0, g_common, 1, None, 0, 0)
    cls_g1 = shared(g_buf, 0, per, g_common, g_half, False, 2, 1)
    cls_d0 = (d_buf, 0, per, 0, d_common, 3, None, 0, 0)
    cls_d1 = shared(d_buf, 0, per, d_common, d_half, False, 4, 2)

    def piece(cls, b, twins=False):
        buf, row0, nrow, col0, ncol, _, _, row1, col1 = cls
        r, k = (row1, col1) if twins else (row0, col0)
        r = pl.multiple_of(b * per + r, 16)
        k = k if isinstance(k, int) else pl.multiple_of(k, 128)
        return buf.at[pl.ds(r, nrow), pl.ds(k, ncol)]

    def hop(cls, s, wait_r, wait_l, send_r, send_l):
        i, k = cls[5], cls[6]
        for d, (b, source, target, wait, send) in enumerate(
            (
                (lax.rem(z - s + nf, nf), left, right, wait_r, send_r),
                (lax.rem(z + s, nf), right, left, wait_l, send_l),
            )
        ):
            ref = piece(cls, b)
            if wait:
                remote(ref, ref, ring_send.at[i], ring_recv.at[i, d, s], source).wait_recv()
            if send:
                remote(ref, ref, ring_send.at[i], ring_recv.at[i, d, s + 1], target).start()
            if wait and k is not None:
                remote(ref, ref, pair_send.at[k], pair_recv.at[k, d, s], twin).start()

    def from_twin(cls, lo, hi):
        k = cls[6]

        def one(s, d):
            b = lax.rem(z - s + nf, nf) if d == 0 else lax.rem(z + s, nf)
            ref = piece(cls, b, True)
            remote(ref, ref, pair_send.at[k], pair_recv.at[k, d, s], twin).wait_recv()

        def body(s, carry):
            one(s, 0)
            one(s, 1)
            return carry

        lax.fori_loop(lo, min(hi, far), body, 0)
        if hi > far:
            one(far, 0)

    classes = [(cls_a, 0), (cls_g0, 0), (cls_g1, 0), (cls_d0, D_START), (cls_d1, D_START)]
    clock = [0]

    def step_kind(s):
        if s < 0 or s > far:
            return None
        if s == 0:
            return (False, False, True, True)
        if s == far - 1:
            return (True, True, True, False)
        if s == far:
            return (True, False, False, False)
        return (True, True, True, True)

    def ticks(n):
        end = min(clock[0] + n, D_START + far + 1)
        while clock[0] < end:
            r = clock[0]
            kinds = [step_kind(r - off) for _, off in classes]
            run = r + 1
            if all(kind is None or kind == (True,) * 4 for kind in kinds):
                while run < end and [step_kind(run - off) for _, off in classes] == kinds:
                    run += 1

                def body(q, carry):
                    for (cls, off), kind in zip(classes, kinds):
                        if kind is not None:
                            hop(cls, q - off, *kind)
                    return carry

                lax.fori_loop(r, run, body, 0)
            else:
                for (cls, off), kind in zip(classes, kinds):
                    if kind is not None:
                        hop(cls, r - off, *kind)
            clock[0] = run

    sent = []

    def put(src, dst, send, recv, i, device):
        copy = remote(src, dst, send.at[i], recv.at[i], device)
        copy.start()
        sent.append(copy)

    def got(dst, send, recv, i, device):
        remote(dst, dst, send.at[i], recv.at[i], device).wait_recv()

    halves = (pl.ds(0, half), pl.ds(half, half))

    def gather_start(buf, send, recv):
        for h in (0, 1):
            part = buf.at[t, halves[h]]
            put(part, part, send, recv, h, xr)
            part = buf.at[t, halves[1 - h]]
            put(part, part, send, recv, 3 - h, xl)
        put(buf.at[t], buf.at[t], send, recv, 6, other)

    def gather_rest(buf, send, recv, pause):
        block_l, block_r, block_o = tp_of(-1, c), tp_of(1, c), tp_of(2, c)
        for i, block, h, source, onward, j in (
            (0, block_l, 0, xl, xr, 4),
            (3, block_r, 1, xr, xl, 5),
            (1, block_l, 1, xl, None, None),
            (2, block_r, 0, xr, None, None),
            (4, block_o, 0, xl, None, None),
            (5, block_o, 1, xr, None, None),
        ):
            if i in (1, 4):
                pause()
            part = buf.at[block, halves[h]]
            got(part, send, recv, i, source)
            if onward is not None:
                put(part, part, send, recv, j, onward)
            put(part, part, send, recv, 7 + i, other)
        pause()
        got(buf.at[tp_of(0, 1 - c)], send, recv, 6, other)
        for i, dx, h in ((0, -1, 0), (1, -1, 1), (2, 1, 0), (3, 1, 1), (4, 2, 0), (5, 2, 1)):
            got(buf.at[tp_of(dx, 1 - c), halves[h]], send, recv, 7 + i, other)

    def reduce_scatter(partial, ship, have, sums, over, last, send, recv, pause):
        for r, dx in enumerate((2, 1, -1, 0)):
            ship[r] = partial(tp_of(dx, 1 - c)).astype(BF16)
            put(ship.at[r], have.at[r], send, recv, r, other)
            own[r] = partial(tp_of(dx, c))
        pause()
        got(have.at[0], send, recv, 0, other)
        sums[0] = (own[0] + have[0].astype(F32)).astype(BF16)
        put(sums.at[0, halves[0]], over.at[0], send, recv, 4, xr)
        put(sums.at[0, halves[1]], over.at[1], send, recv, 5, xl)
        got(have.at[1], send, recv, 1, other)
        sums[1, halves[1]] = (own[1, halves[1]] + have[1, halves[1]].astype(F32)).astype(BF16)
        put(sums.at[1, halves[1]], last.at[0, halves[1]], send, recv, 6, xr)
        got(have.at[2], send, recv, 2, other)
        sums[2, halves[0]] = (own[2, halves[0]] + have[2, halves[0]].astype(F32)).astype(BF16)
        put(sums.at[2, halves[0]], last.at[1, halves[0]], send, recv, 7, xl)
        got(have.at[3], send, recv, 3, other)
        own[3] = own[3] + have[3].astype(F32)
        pause()
        got(over.at[0], send, recv, 4, xl)
        sums[1, halves[0]] = (own[1, halves[0]] + have[1, halves[0]].astype(F32) + over[0].astype(F32)).astype(BF16)
        put(sums.at[1, halves[0]], last.at[0, halves[0]], send, recv, 8, xr)
        got(over.at[1], send, recv, 5, xr)
        sums[2, halves[1]] = (own[2, halves[1]] + have[2, halves[1]].astype(F32) + over[1].astype(F32)).astype(BF16)
        put(sums.at[2, halves[1]], last.at[1, halves[1]], send, recv, 9, xl)
        pause()
        got(last.at[0, halves[1]], send, recv, 6, xl)
        got(last.at[1, halves[0]], send, recv, 7, xr)
        got(last.at[0, halves[0]], send, recv, 8, xl)
        got(last.at[1, halves[1]], send, recv, 9, xr)
        return own[3] + last[0].astype(F32) + last[1].astype(F32)

    def normalize(source, gain):
        total = jnp.zeros((rows, 1), F32)
        for j in range(nt):
            v = source[j].astype(F32)
            total = total + jnp.sum(v * v, axis=-1, keepdims=True)
        scale = lax.rsqrt(total * (1.0 / (nt * width)) + NORM_EPS)
        for j in range(nt):
            span = pl.ds(j * width, width)
            nrm[:, span] = (source[j].astype(F32) * scale * gain[:, span]).astype(BF16)

    for copy in copies[1:6]:
        copy.wait()
    hop(cls_a, 0, False, False, True, True)
    copies[0].wait()
    gather_start(tok_all, tok_send, tok_recv)
    for copy in copies[6:]:
        copy.wait()
    hop(cls_g0, 0, False, False, True, True)
    hop(cls_g1, 0, False, False, True, True)
    clock[0] = 1

    n_id = lax.broadcasted_iota(jnp.int32, (128, rows), 0)
    m_id = lax.broadcasted_iota(jnp.int32, (128, rows), 1)
    lane = lax.broadcasted_iota(jnp.int32, (rows, 2 * HEAD), 1)
    low_head = lane < HEAD
    fwd = jax.nn.log_sigmoid(fdec[...])
    bwd = jax.nn.log_sigmoid(bdec[...])
    for h in range(2):
        for chunk in range(rows // 128):
            gap = (n_id + (chunk * 128) - m_id).astype(F32)
            exponent = jnp.where(gap >= 0, fwd[:, h : h + 1] * gap, bwd[:, h : h + 1] * (-gap))
            decay[h, pl.ds(chunk * 128, 128), :] = jnp.exp(exponent)
    ticks(1)
    gather_rest(tok_all, tok_send, tok_recv, lambda: ticks(1))
    normalize(tok_all, gain1)

    first = lax.div(z, tiles)

    def add_group(k, start=False):
        j = lax.rem(first + k + nt, nt)
        rows_j = pl.ds(pl.multiple_of(j * width, width), width)
        term = jnp.dot(
            nrm[:, pl.ds(pl.multiple_of(j * width, width), width)], a_buf[rows_j, pl.ds(0, mcol)], preferred_element_type=F32
        )
        qacc[...] = term if start else qacc[...] + term

    for k in range(far // tiles):
        ticks(tiles * k + tiles + 1 - clock[0])
        if k == 0:
            from_twin(cls_a, 1, tiles)
            add_group(0, True)
        else:
            from_twin(cls_a, tiles * k, tiles * k + tiles)
            add_group(k)
            add_group(-k)
    ticks(far + 1 - clock[0])
    from_twin(cls_a, far, far + 1)
    add_group(far // tiles)
    qkvg[...] = qacc[...].astype(BF16)
    ticks(1)

    def rotated(n):
        v = qkvg[:, pl.ds(n * cols, cols)].astype(F32)
        lo_half = lax.rem(lane, HEAD) < HEAD // 2
        swapped = jnp.where(lo_half, pltpu.roll(v, 2 * HEAD - HEAD // 2, 1), pltpu.roll(v, HEAD // 2, 1))
        return v * cos[...] + swapped * sin[...]

    rq = rotated(0)
    rk = (rotated(1) * HEAD**-0.5).astype(BF16)
    value = qkvg[:, pl.ds(2 * cols, cols)]
    kept = []
    for h in range(2):
        q_h = jnp.where(low_head if h == 0 else jnp.logical_not(low_head), rq, 0.0).astype(BF16)
        parts = []
        for chunk in range(rows // 128):
            scores = lax.dot_general(q_h[chunk * 128 : (chunk + 1) * 128], rk, NT_DIMS, preferred_element_type=F32)
            weighted = (scores * decay[h, pl.ds(chunk * 128, 128), :]).astype(BF16)
            parts.append(jnp.dot(weighted, value, preferred_element_type=F32))
        kept.append(jnp.concatenate(parts, axis=0))
    ticks(1)
    retained = jnp.where(low_head, kept[0], kept[1])

    def head_mean(v):
        lo = jnp.sum(jnp.where(low_head, v, 0.0), axis=-1, keepdims=True)
        hi = jnp.sum(jnp.where(low_head, 0.0, v), axis=-1, keepdims=True)
        return jnp.where(low_head, lo, hi) * (1.0 / HEAD)

    centered = retained - head_mean(retained)
    normalized = centered * lax.rsqrt(head_mean(centered * centered) + GROUP_EPS)
    gate = qkvg[:, pl.ds(3 * cols, cols)].astype(F32)
    mixed[...] = (gate / (1.0 + jnp.exp(-gate)) * normalized).astype(BF16)

    def merge_part(j):
        w = a_buf[pl.ds(pl.multiple_of(j * width, width), width), pl.ds(mcol, wm.shape[1])]
        return lax.dot_general(mixed[...], w, NT_DIMS, preferred_element_type=F32)

    merged = reduce_scatter(merge_part, ship1, got1, sums1, over1, last1, rs1_send, rs1_recv, lambda: ticks(1))
    mid_all[t] = (tok_all[t].astype(F32) + merged).astype(BF16)
    gather_start(mid_all, mid_send, mid_recv)
    gather_rest(mid_all, mid_send, mid_recv, lambda: ticks(1))
    normalize(mid_all, gain2)
    from_twin(cls_g1, 1, far + 1)
    acts[:, pl.ds(0, ff)] = jnp.dot(nrm[...], g_buf[:, pl.ds(0, ff)], preferred_element_type=F32)
    ticks(1)
    acts[:, pl.ds(ff, ff)] = jnp.dot(nrm[...], g_buf[:, pl.ds(ff, ff)], preferred_element_type=F32)
    ticks(1)
    gated = acts[:, pl.ds(0, ff)]
    hid[...] = (gated / (1.0 + jnp.exp(-gated)) * acts[:, pl.ds(ff, ff)]).astype(BF16)
    ticks(D_START + far + 1)
    from_twin(cls_d1, 1, far + 1)

    def down_part(j):
        w = d_buf[pl.ds(pl.multiple_of(j * width, width), width), :]
        return lax.dot_general(hid[...], w, NT_DIMS, preferred_element_type=F32)

    summed = reduce_scatter(down_part, ship2, got2, sums2, over2, last2, rs2_send, rs2_recv, lambda: None)
    out[...] = (mid_all[t].astype(F32) + summed).astype(BF16)

    for cls, _ in classes:
        buf, row0, nrow, col0, ncol, i, k, _, _ = cls
        cut = pl.ds(col0 if isinstance(col0, int) else pl.multiple_of(col0, 128), ncol)
        whole = buf.at[pl.ds(0, (nf - 1) * nrow), cut]
        remote(whole, whole, ring_send.at[i], ring_recv.at[i, 0, 0], right).wait_send()
        if k is not None:
            remote(whole, whole, pair_send.at[k], pair_recv.at[k, 0, 0], twin).wait_send()
    for copy in sent:
        copy.wait_send()


def on_device(nf, nt, tokens, input_gain, wq, wk, wv, wo, fdec, bdec, wm, middle_gain, wgate, wup, wdown):
    seqs, rows, width = tokens.shape
    per, cols = wq.shape
    ff = wgate.shape[1]
    full = nf * per
    nx = nt // 2
    cos, sin = rotation_tables(rows)
    anywhere = pl.BlockSpec(memory_space=pl.ANY)
    vmem = pl.BlockSpec(memory_space=pltpu.VMEM)
    dma = pltpu.SemaphoreType.DMA
    block = (rows, width)
    exchange = [
        pltpu.VMEM((nx, *block), BF16),
        pltpu.VMEM((nx, *block), BF16),
        pltpu.VMEM((3, *block), BF16),
        pltpu.VMEM((2, rows // 2, width), BF16),
        pltpu.VMEM((2, *block), BF16),
    ]
    out = pl.pallas_call(
        functools.partial(layer_kernel, nf, nt),
        out_shape=jax.ShapeDtypeStruct(block, BF16),
        in_specs=[anywhere, vmem]
        + [anywhere] * 4
        + [vmem, vmem, anywhere, vmem]
        + [anywhere] * 3
        + [vmem, vmem],
        out_specs=vmem,
        scratch_shapes=[
            pltpu.VMEM((full, 4 * cols + wm.shape[0]), BF16),
            pltpu.VMEM((full, 2 * ff), BF16),
            pltpu.VMEM((full, ff), BF16),
            pltpu.VMEM((nt, *block), BF16),
            pltpu.VMEM((nt, *block), BF16),
            pltpu.VMEM((rows, full), BF16),
            pltpu.VMEM((2, rows, rows), F32),
            pltpu.VMEM((rows, 4 * cols), F32),
            pltpu.VMEM((rows, 4 * cols), BF16),
            pltpu.VMEM((rows, cols), BF16),
            pltpu.VMEM((rows, 2 * ff), F32),
            pltpu.VMEM((rows, ff), BF16),
            pltpu.VMEM((nx, *block), F32),
            *exchange,
            *exchange,
            dma((9,)),
            dma((5,)),
            dma((5, 2, nf // 2 + 1)),
            dma((3,)),
            dma((3, 2, nf // 2 + 1)),
            dma((13,)),
            dma((13,)),
            dma((13,)),
            dma((13,)),
            dma((10,)),
            dma((10,)),
            dma((10,)),
            dma((10,)),
        ],
        compiler_params=pltpu.CompilerParams(
            collective_id=0, has_side_effects=True, vmem_limit_bytes=60 * 1024 * 1024
        ),
    )(
        tokens.reshape(seqs * rows, width),
        input_gain.reshape(1, -1),
        wq,
        wk,
        wv,
        wo,
        fdec.reshape(1, -1),
        bdec.reshape(1, -1),
        wm.T,
        middle_gain.reshape(1, -1),
        wgate,
        wup,
        wdown.T,
        jnp.asarray(cos),
        jnp.asarray(sin),
    )
    return out.reshape(seqs, rows, width)


def solution(mesh):
    sizes = dict(mesh.shape)
    placed = (
        P(("grp", "fs"), None, "tp"),
        P(),
        P("fs", "tp"),
        P("fs", "tp"),
        P("fs", "tp"),
        P("fs", "tp"),
        P("tp"),
        P("tp"),
        P("tp", "fs"),
        P(),
        P("fs", "tp"),
        P("fs", "tp"),
        P("tp", "fs"),
    )
    return jax.shard_map(
        functools.partial(on_device, sizes["fs"], sizes["tp"]),
        mesh=mesh,
        in_specs=placed,
        out_specs=P(("grp", "fs"), None, "tp"),
        check_vma=False,
    )
```

```python
import functools

import jax
import jax.numpy as jnp
import numpy as np
from jax import lax
from jax.experimental import pallas as pl
from jax.experimental.pallas import tpu as pltpu
from jax.sharding import PartitionSpec as P

MESH = pl.DeviceIdType.MESH
HEAD = 64
NORM_EPS = 1e-06
GROUP_EPS = 1e-05
ROPE_BASE = 10000.0
F32 = jnp.float32
BF16 = jnp.bfloat16

D_START = 0
SLOTS = 4
STRIDE = 3

NT_DIMS = (((1,), (1,)), ((), ()))


def rotation_tables(length):
    half = HEAD // 2
    inverse = ROPE_BASE ** (-np.arange(half, dtype=np.float32) / np.float32(half))
    angles = np.arange(length, dtype=np.float32)[:, None] * inverse.astype(np.float32)[None, :]
    cosine, sine = np.cos(angles), np.sin(angles)
    return (
        np.concatenate([cosine, cosine] * 2, axis=1).astype(np.float32),
        np.concatenate([-sine, sine] * 2, axis=1).astype(np.float32),
    )


def remote(src, dst, send_sem, recv_sem, device):
    return pltpu.make_async_remote_copy(
        src_ref=src, dst_ref=dst, send_sem=send_sem, recv_sem=recv_sem, device_id=device, device_id_type=MESH
    )


def layer_kernel(
    nf,
    nt,
    tok,
    gain1,
    wq,
    wk,
    wv,
    wo,
    fdec,
    bdec,
    wm,
    gain2,
    wgate,
    wup,
    wdown,
    cos,
    sin,
    out,
    a_buf,
    g_buf,
    d_buf,
    tok_all,
    mid_all,
    nrm,
    decay,
    qacc,
    qkvg,
    mixed,
    acts,
    hid,
    own,
    ship1,
    got1,
    sums1,
    over1,
    last1,
    ship2,
    got2,
    sums2,
    over2,
    last2,
    local_sem,
    far_send,
    far_recv,
    far_pair_send,
    far_pair_recv,
    ring_send,
    ring_recv,
    pair_send,
    pair_recv,
    tok_send,
    tok_recv,
    mid_send,
    mid_recv,
    rs1_send,
    rs1_recv,
    rs2_send,
    rs2_recv,
):
    g = lax.axis_index("grp")
    z = lax.axis_index("fs")
    t = lax.axis_index("tp")
    nx = nt // 2
    x, c = lax.div(t, 2), lax.rem(t, 2)
    parity = lax.rem(g, 2)
    twin = {"grp": g + 1 - 2 * parity}
    right, left = {"fs": lax.rem(z + 1, nf)}, {"fs": lax.rem(z + nf - 1, nf)}
    right_far, left_far = {"fs": lax.rem(z + STRIDE, nf)}, {"fs": lax.rem(z + nf - STRIDE, nf)}

    def tp_of(dx, core):
        return lax.rem(x + dx + nx, nx) * 2 + core

    xr, xl, other = {"tp": tp_of(1, c)}, {"tp": tp_of(-1, c)}, {"tp": tp_of(0, 1 - c)}
    far = nf // 2
    rows, width = tok.shape
    half = rows // 2
    per, cols = wq.shape
    ff = wgate.shape[1]
    mcol = 4 * cols
    tiles = width // per

    mine = pl.ds(pl.multiple_of(z * per, per), per)
    copies = [pltpu.make_async_copy(tok, tok_all.at[t], local_sem.at[0])]
    for n, w in enumerate((wq, wk, wv, wo, wm)):
        copies.append(pltpu.make_async_copy(w, a_buf.at[mine, pl.ds(n * cols, cols)], local_sem.at[1 + n]))
    copies.append(pltpu.make_async_copy(wgate, g_buf.at[mine, pl.ds(0, ff)], local_sem.at[6]))
    copies.append(pltpu.make_async_copy(wup, g_buf.at[mine, pl.ds(ff, ff)], local_sem.at[7]))
    copies.append(pltpu.make_async_copy(wdown, d_buf.at[mine, :], local_sem.at[8]))
    for copy in copies:
        copy.start()

    barrier = pltpu.get_barrier_semaphore()
    for peer in (left, right, left_far, right_far, xl, xr, other, twin):
        pl.semaphore_signal(barrier, inc=1, device_id=peer, device_id_type=MESH)
    pl.semaphore_wait(barrier, 8)

    def shared(buf, row0, nrow, col0, ncol, by_row, i, k):
        step_r, step_c = (nrow, 0) if by_row else (0, ncol)
        flip = 1 - parity
        return (buf, row0 + step_r * parity, nrow, col0 + step_c * parity, ncol, i, k, row0 + step_r * flip, col0 + step_c * flip)

    g_common, g_half = 4 * 128, 3 * 128
    d_common, d_half = 128, 2 * 128
    lower = per // 2
    cls_a = shared(a_buf, 0, lower, 0, mcol + wm.shape[1], True, None, None)
    cls_g = shared(g_buf, 0, per, g_common, g_half, False, None, 0)
    cls_d = shared(d_buf, 0, per, d_common, d_half, False, 5, 1)
    cls_g0 = (g_buf, 0, lower, 0, g_common, 0, None, 0, 0)
    cls_g1 = (g_buf, lower, lower, 0, g_common, 1, None, 0, 0)
    cls_g2 = shared(g_buf, 0, lower, g_common, g_half, False, 2, None)
    cls_g3 = shared(g_buf, lower, lower, g_common, g_half, False, 3, None)
    cls_d0 = (d_buf, 0, per, 0, d_common, 4, None, 0, 0)
    paired = {3: cls_g, 5: cls_d}

    def piece(cls, b, twins=False):
        buf, row0, nrow, col0, ncol, _, _, row1, col1 = cls
        r, k = (row1, col1) if twins else (row0, col0)
        r = pl.multiple_of(b * per + r, 16)
        k = k if isinstance(k, int) else pl.multiple_of(k, 128)
        return buf.at[pl.ds(r, nrow), pl.ds(k, ncol)]

    def hop(cls, s, wait_r, wait_l, send_r, send_l):
        i = cls[5]
        for d, (b, source, target, wait, send) in enumerate(
            (
                (lax.rem(z - s + nf, nf), left, right, wait_r, send_r),
                (lax.rem(z + s, nf), right, left, wait_l, send_l),
            )
        ):
            ref = piece(cls, b)
            if wait:
                remote(ref, ref, ring_send.at[i], ring_recv.at[i, d, lax.rem(s, SLOTS)], source).wait_recv()
            if send:
                remote(ref, ref, ring_send.at[i], ring_recv.at[i, d, lax.rem(s + 1, SLOTS)], target).start()
            if wait and i in paired:
                ref, k = piece(paired[i], b), paired[i][6]
                remote(ref, ref, pair_send.at[k], pair_recv.at[k, d, s], twin).start()

    def from_twin(cls, lo, hi):
        k = cls[6]

        def one(s, d):
            b = lax.rem(z - s + nf, nf) if d == 0 else lax.rem(z + s, nf)
            ref = piece(cls, b, True)
            remote(ref, ref, pair_send.at[k], pair_recv.at[k, d, s], twin).wait_recv()

        def body(s, carry):
            one(s, 0)
            one(s, 1)
            return carry

        lax.fori_loop(lo, min(hi, far), body, 0)
        if hi > far:
            one(far, 0)

    stages = (far - 1) // STRIDE

    def at_distance(d, twins=False):
        return piece(cls_a, lax.rem(z - d + nf, nf), twins)

    def pass_on(d, step, device):
        ref = at_distance(d)
        remote(ref, ref, far_send.at[0], far_recv.at[d + step + far - 1], device).start()

    def receive(d):
        ref = at_distance(d)
        remote(ref, ref, far_send.at[0], far_recv.at[d + far - 1], right).wait_recv()

    def to_twin(d):
        ref = at_distance(d)
        remote(ref, ref, far_pair_send.at[0], far_pair_recv.at[d + far - 1], twin).start()

    def twin_blocks(lo, hi):
        for dist in range(lo, hi):
            for d in (dist, -dist) if dist < far else (dist,):
                ref = at_distance(d, True)
                remote(ref, ref, far_pair_send.at[0], far_pair_recv.at[d + far - 1], twin).wait_recv()

    def stage(i):
        for sign, ahead, behind, jump in ((1, right, left, right_far), (-1, left, right, left_far)):
            d = sign * STRIDE * i
            if i > 0:
                receive(d)
            if i < stages:
                pass_on(d, sign * STRIDE, jump)
            if abs(d) + 1 < far or sign > 0:
                pass_on(d, sign, ahead)
            if i > 0:
                pass_on(d, -sign, behind)
                to_twin(d)

    def fills(i):
        near = [1, -1] if i == 0 else [STRIDE * i - 1, 1 - STRIDE * i, STRIDE * i + 1, -STRIDE * i - 1]
        for d in near:
            if d > -far:
                receive(d)
                to_twin(d)

    classes = [(cls_g0, 0), (cls_g1, 0), (cls_g2, 0), (cls_g3, 0), (cls_d0, D_START), (cls_d, D_START)]
    clock = [0]

    def step_kind(s):
        if s < 0 or s > far:
            return None
        if s == 0:
            return (False, False, True, True)
        if s == far - 1:
            return (True, True, True, False)
        if s == far:
            return (True, False, False, False)
        return (True, True, True, True)

    def ticks(n):
        end = min(clock[0] + n, D_START + far + 1)
        while clock[0] < end:
            r = clock[0]
            kinds = [step_kind(r - off) for _, off in classes]
            run = r + 1
            if all(kind is None or kind == (True,) * 4 for kind in kinds):
                while run < end and [step_kind(run - off) for _, off in classes] == kinds:
                    run += 1

                def body(q, carry):
                    for (cls, off), kind in zip(classes, kinds):
                        if kind is not None:
                            hop(cls, q - off, *kind)
                    return carry

                lax.fori_loop(r, run, body, 0)
            else:
                for (cls, off), kind in zip(classes, kinds):
                    if kind is not None:
                        hop(cls, r - off, *kind)
            clock[0] = run

    def put(src, dst, send, recv, i, device):
        remote(src, dst, send.at[0], recv.at[i], device).start()

    def got(dst, send, recv, i, device):
        remote(dst, dst, send.at[0], recv.at[i], device).wait_recv()

    halves = (pl.ds(0, half), pl.ds(half, half))

    def gather_start(buf, send, recv):
        for h in (0, 1):
            part = buf.at[t, halves[h]]
            put(part, part, send, recv, h, xr)
            part = buf.at[t, halves[1 - h]]
            put(part, part, send, recv, 3 - h, xl)
        put(buf.at[t], buf.at[t], send, recv, 6, other)

    def gather_rest(buf, send, recv, pause):
        block_l, block_r, block_o = tp_of(-1, c), tp_of(1, c), tp_of(2, c)
        for i, block, h, source, onward, j in (
            (0, block_l, 0, xl, xr, 4),
            (3, block_r, 1, xr, xl, 5),
            (1, block_l, 1, xl, None, None),
            (2, block_r, 0, xr, None, None),
            (4, block_o, 0, xl, None, None),
            (5, block_o, 1, xr, None, None),
        ):
            if i in (1, 4):
                pause()
            part = buf.at[block, halves[h]]
            got(part, send, recv, i, source)
            if onward is not None:
                put(part, part, send, recv, j, onward)
            put(part, part, send, recv, 7 + i, other)
        pause()
        got(buf.at[tp_of(0, 1 - c)], send, recv, 6, other)
        for i, dx, h in ((0, -1, 0), (1, -1, 1), (2, 1, 0), (3, 1, 1), (4, 2, 0), (5, 2, 1)):
            got(buf.at[tp_of(dx, 1 - c), halves[h]], send, recv, 7 + i, other)

    def reduce_scatter(partial, ship, have, sums, over, last, send, recv, pause):
        def product(r, dx):
            ship[r] = partial(tp_of(dx, 1 - c)).astype(BF16)
            put(ship.at[r], have.at[r], send, recv, r, other)
            own[r] = partial(tp_of(dx, c))

        product(0, 2)
        product(1, 1)
        got(have.at[0], send, recv, 0, other)
        sums[0] = (own[0] + have[0].astype(F32)).astype(BF16)
        put(sums.at[0, halves[0]], over.at[0], send, recv, 4, xr)
        put(sums.at[0, halves[1]], over.at[1], send, recv, 5, xl)
        product(2, -1)
        got(have.at[1], send, recv, 1, other)
        sums[1, halves[1]] = (own[1, halves[1]] + have[1, halves[1]].astype(F32)).astype(BF16)
        put(sums.at[1, halves[1]], last.at[0, halves[1]], send, recv, 6, xr)
        product(3, 0)
        got(have.at[2], send, recv, 2, other)
        sums[2, halves[0]] = (own[2, halves[0]] + have[2, halves[0]].astype(F32)).astype(BF16)
        put(sums.at[2, halves[0]], last.at[1, halves[0]], send, recv, 7, xl)
        pause()
        got(have.at[3], send, recv, 3, other)
        own[3] = own[3] + have[3].astype(F32)
        pause()
        got(over.at[0], send, recv, 4, xl)
        sums[1, halves[0]] = (own[1, halves[0]] + have[1, halves[0]].astype(F32) + over[0].astype(F32)).astype(BF16)
        put(sums.at[1, halves[0]], last.at[0, halves[0]], send, recv, 8, xr)
        got(over.at[1], send, recv, 5, xr)
        sums[2, halves[1]] = (own[2, halves[1]] + have[2, halves[1]].astype(F32) + over[1].astype(F32)).astype(BF16)
        put(sums.at[2, halves[1]], last.at[1, halves[1]], send, recv, 9, xl)
        pause()
        got(last.at[0, halves[1]], send, recv, 6, xl)
        got(last.at[1, halves[0]], send, recv, 7, xr)
        got(last.at[0, halves[0]], send, recv, 8, xl)
        got(last.at[1, halves[1]], send, recv, 9, xr)
        return own[3] + last[0].astype(F32) + last[1].astype(F32)

    def normalize(source, gain):
        total = jnp.zeros((rows, 1), F32)
        for j in range(nt):
            v = source[j].astype(F32)
            total = total + jnp.sum(v * v, axis=-1, keepdims=True)
        scale = lax.rsqrt(total * (1.0 / (nt * width)) + NORM_EPS)
        for j in range(nt):
            span = pl.ds(j * width, width)
            nrm[:, span] = (source[j].astype(F32) * scale * gain[:, span]).astype(BF16)

    first = lax.div(z, tiles)

    def add_group(k, start=False):
        j = lax.rem(first + k + nt, nt)
        rows_j = pl.ds(pl.multiple_of(j * width, width), width)
        term = jnp.dot(
            nrm[:, pl.ds(pl.multiple_of(j * width, width), width)], a_buf[rows_j, pl.ds(0, mcol)], preferred_element_type=F32
        )
        qacc[...] = term if start else qacc[...] + term

    n_id = lax.broadcasted_iota(jnp.int32, (128, rows), 0)
    m_id = lax.broadcasted_iota(jnp.int32, (128, rows), 1)
    lane = lax.broadcasted_iota(jnp.int32, (rows, 2 * HEAD), 1)
    low_head = lane < HEAD

    def decay_weights(h):
        fwd = jax.nn.log_sigmoid(fdec[...])
        bwd = jax.nn.log_sigmoid(bdec[...])
        for chunk in range(rows // 128):
            gap = (n_id + (chunk * 128) - m_id).astype(F32)
            exponent = jnp.where(gap >= 0, fwd[:, h : h + 1] * gap, bwd[:, h : h + 1] * (-gap))
            decay[h, pl.ds(chunk * 128, 128), :] = jnp.exp(exponent)

    for copy in copies[1:6]:
        copy.wait()
    stage(0)
    copies[0].wait()
    gather_start(tok_all, tok_send, tok_recv)
    for copy in copies[6:]:
        copy.wait()
    ticks(1)
    decay_weights(0)
    stage(1)
    ticks(1)
    fills(0)
    decay_weights(1)
    stage(2)
    ticks(1)
    fills(1)
    gather_rest(tok_all, tok_send, tok_recv, lambda: None)
    ticks(1)
    stage(3)
    ticks(1)
    fills(2)
    normalize(tok_all, gain1)
    ticks(1)
    stage(4)
    ticks(1)
    fills(3)
    twin_blocks(1, 2 * tiles)
    add_group(0, True)
    ticks(1)
    stage(5)
    ticks(1)
    fills(4)
    add_group(1)
    add_group(-1)
    fills(5)
    ticks(1)
    twin_blocks(2 * tiles, 3 * tiles)
    add_group(2)
    add_group(-2)
    twin_blocks(3 * tiles, far + 1)
    add_group(3)
    add_group(-3)
    add_group(far // tiles)
    qkvg[...] = qacc[...].astype(BF16)
    ticks(1)

    def rotated(n):
        v = qkvg[:, pl.ds(n * cols, cols)].astype(F32)
        lo_half = lax.rem(lane, HEAD) < HEAD // 2
        swapped = jnp.where(lo_half, pltpu.roll(v, 2 * HEAD - HEAD // 2, 1), pltpu.roll(v, HEAD // 2, 1))
        return v * cos[...] + swapped * sin[...]

    rq = rotated(0)
    rk = (rotated(1) * HEAD**-0.5).astype(BF16)
    value = qkvg[:, pl.ds(2 * cols, cols)]
    kept = []
    for h in range(2):
        q_h = jnp.where(low_head if h == 0 else jnp.logical_not(low_head), rq, 0.0).astype(BF16)
        parts = []
        for chunk in range(rows // 128):
            scores = lax.dot_general(q_h[chunk * 128 : (chunk + 1) * 128], rk, NT_DIMS, preferred_element_type=F32)
            weighted = (scores * decay[h, pl.ds(chunk * 128, 128), :]).astype(BF16)
            parts.append(jnp.dot(weighted, value, preferred_element_type=F32))
        kept.append(jnp.concatenate(parts, axis=0))
    ticks(1)
    retained = jnp.where(low_head, kept[0], kept[1])

    def head_mean(v):
        lo = jnp.sum(jnp.where(low_head, v, 0.0), axis=-1, keepdims=True)
        hi = jnp.sum(jnp.where(low_head, 0.0, v), axis=-1, keepdims=True)
        return jnp.where(low_head, lo, hi) * (1.0 / HEAD)

    centered = retained - head_mean(retained)
    normalized = centered * lax.rsqrt(head_mean(centered * centered) + GROUP_EPS)
    gate = qkvg[:, pl.ds(3 * cols, cols)].astype(F32)
    mixed[...] = (gate / (1.0 + jnp.exp(-gate)) * normalized).astype(BF16)

    def merge_part(j):
        w = a_buf[pl.ds(pl.multiple_of(j * width, width), width), pl.ds(mcol, wm.shape[1])]
        return lax.dot_general(mixed[...], w, NT_DIMS, preferred_element_type=F32)

    merged = reduce_scatter(merge_part, ship1, got1, sums1, over1, last1, rs1_send, rs1_recv, lambda: ticks(1))
    mid_all[t] = (tok_all[t].astype(F32) + merged).astype(BF16)
    gather_start(mid_all, mid_send, mid_recv)
    gather_rest(mid_all, mid_send, mid_recv, lambda: ticks(1))
    normalize(mid_all, gain2)
    ticks(far + 1 - clock[0])
    from_twin(cls_g, 1, far + 1)
    acts[:, pl.ds(0, ff)] = jnp.dot(nrm[...], g_buf[:, pl.ds(0, ff)], preferred_element_type=F32)
    ticks(1)
    acts[:, pl.ds(ff, ff)] = jnp.dot(nrm[...], g_buf[:, pl.ds(ff, ff)], preferred_element_type=F32)
    ticks(1)
    gated = acts[:, pl.ds(0, ff)]
    hid[...] = (gated / (1.0 + jnp.exp(-gated)) * acts[:, pl.ds(ff, ff)]).astype(BF16)
    ticks(D_START + far + 1)
    from_twin(cls_d, 1, far + 1)

    def down_part(j):
        w = d_buf[pl.ds(pl.multiple_of(j * width, width), width), :]
        return lax.dot_general(hid[...], w, NT_DIMS, preferred_element_type=F32)

    summed = reduce_scatter(down_part, ship2, got2, sums2, over2, last2, rs2_send, rs2_recv, lambda: None)
    out[...] = (mid_all[t].astype(F32) + summed).astype(BF16)

    whole = a_buf.at[pl.ds(0, (nf - 1) * (per // 2)), :]
    remote(whole, whole, far_send.at[0], far_recv.at[0], right).wait_send()
    remote(whole, whole, far_pair_send.at[0], far_pair_recv.at[0], twin).wait_send()
    def drain(cls, sem, recv, device):
        buf, row0, nrow, col0, ncol = cls[:5]
        cut = pl.ds(col0 if isinstance(col0, int) else pl.multiple_of(col0, 128), ncol)
        total = buf.at[pl.ds(0, (nf - 1) * nrow), cut]
        remote(total, total, sem, recv, device).wait_send()

    for cls, _ in classes:
        drain(cls, ring_send.at[cls[5]], ring_recv.at[cls[5], 0, 0], right)
    for cls in paired.values():
        drain(cls, pair_send.at[cls[6]], pair_recv.at[cls[6], 0, 0], twin)
    whole = tok_all.at[pl.ds(0, nt - 1)]
    for sem in (tok_send, mid_send, rs1_send, rs2_send):
        remote(whole, whole, sem.at[0], tok_recv.at[0], other).wait_send()


def on_device(nf, nt, tokens, input_gain, wq, wk, wv, wo, fdec, bdec, wm, middle_gain, wgate, wup, wdown):
    seqs, rows, width = tokens.shape
    per, cols = wq.shape
    ff = wgate.shape[1]
    full = nf * per
    nx = nt // 2
    cos, sin = rotation_tables(rows)
    anywhere = pl.BlockSpec(memory_space=pl.ANY)
    vmem = pl.BlockSpec(memory_space=pltpu.VMEM)
    dma = pltpu.SemaphoreType.DMA
    block = (rows, width)
    exchange = [
        pltpu.VMEM((nx, *block), BF16),
        pltpu.VMEM((nx, *block), BF16),
        pltpu.VMEM((3, *block), BF16),
        pltpu.VMEM((2, rows // 2, width), BF16),
        pltpu.VMEM((2, *block), BF16),
    ]
    out = pl.pallas_call(
        functools.partial(layer_kernel, nf, nt),
        out_shape=jax.ShapeDtypeStruct(block, BF16),
        in_specs=[anywhere, vmem]
        + [anywhere] * 4
        + [vmem, vmem, anywhere, vmem]
        + [anywhere] * 3
        + [vmem, vmem],
        out_specs=vmem,
        scratch_shapes=[
            pltpu.VMEM((full, 4 * cols + wm.shape[0]), BF16),
            pltpu.VMEM((full, 2 * ff), BF16),
            pltpu.VMEM((full, ff), BF16),
            pltpu.VMEM((nt, *block), BF16),
            pltpu.VMEM((nt, *block), BF16),
            pltpu.VMEM((rows, full), BF16),
            pltpu.VMEM((2, rows, rows), F32),
            pltpu.VMEM((rows, 4 * cols), F32),
            pltpu.VMEM((rows, 4 * cols), BF16),
            pltpu.VMEM((rows, cols), BF16),
            pltpu.VMEM((rows, 2 * ff), F32),
            pltpu.VMEM((rows, ff), BF16),
            pltpu.VMEM((nx, *block), F32),
            *exchange,
            *exchange,
            dma((9,)),
            dma((1,)),
            dma((nf,)),
            dma((1,)),
            dma((nf,)),
            dma((6,)),
            dma((6, 2, SLOTS)),
            dma((2,)),
            dma((2, 2, nf // 2 + 1)),
            dma((1,)),
            dma((13,)),
            dma((1,)),
            dma((13,)),
            dma((1,)),
            dma((10,)),
            dma((1,)),
            dma((10,)),
        ],
        compiler_params=pltpu.CompilerParams(
            collective_id=0, has_side_effects=True, vmem_limit_bytes=60 * 1024 * 1024
        ),
    )(
        tokens.reshape(seqs * rows, width),
        input_gain.reshape(1, -1),
        wq,
        wk,
        wv,
        wo,
        fdec.reshape(1, -1),
        bdec.reshape(1, -1),
        wm.T,
        middle_gain.reshape(1, -1),
        wgate,
        wup,
        wdown.T,
        jnp.asarray(cos),
        jnp.asarray(sin),
    )
    return out.reshape(seqs, rows, width)


def solution(mesh):
    sizes = dict(mesh.shape)
    placed = (
        P(("grp", "fs"), None, "tp"),
        P(),
        P("fs", "tp"),
        P("fs", "tp"),
        P("fs", "tp"),
        P("fs", "tp"),
        P("tp"),
        P("tp"),
        P("tp", "fs"),
        P(),
        P("fs", "tp"),
        P("fs", "tp"),
        P("tp", "fs"),
    )
    return jax.shard_map(
        functools.partial(on_device, sizes["fs"], sizes["tp"]),
        mesh=mesh,
        in_specs=placed,
        out_specs=P(("grp", "fs"), None, "tp"),
        check_vma=False,
    )
```

```python
import functools

import jax
import jax.numpy as jnp
import numpy as np
from jax import lax
from jax.experimental import pallas as pl
from jax.experimental.pallas import tpu as pltpu
from jax.sharding import PartitionSpec as P

MESH = pl.DeviceIdType.MESH
HEAD = 64
NORM_EPS = 1e-06
GROUP_EPS = 1e-05
ROPE_BASE = 10000.0
F32 = jnp.float32
BF16 = jnp.bfloat16

D_START = 0
SLOTS = 4
STRIDE = 3

NT_DIMS = (((1,), (1,)), ((), ()))


def rotation_tables(length):
    half = HEAD // 2
    inverse = ROPE_BASE ** (-np.arange(half, dtype=np.float32) / np.float32(half))
    angles = np.arange(length, dtype=np.float32)[:, None] * inverse.astype(np.float32)[None, :]
    cosine, sine = np.cos(angles), np.sin(angles)
    return (
        np.concatenate([cosine, cosine] * 2, axis=1).astype(np.float32),
        np.concatenate([-sine, sine] * 2, axis=1).astype(np.float32),
    )


def remote(src, dst, send_sem, recv_sem, device):
    return pltpu.make_async_remote_copy(
        src_ref=src, dst_ref=dst, send_sem=send_sem, recv_sem=recv_sem, device_id=device, device_id_type=MESH
    )


def layer_kernel(
    nf,
    nt,
    tok,
    gain1,
    wq,
    wk,
    wv,
    wo,
    fdec,
    bdec,
    wm,
    gain2,
    wgate,
    wup,
    wdown,
    cos,
    sin,
    out,
    a_buf,
    g_buf,
    d_buf,
    tok_all,
    mid_all,
    nrm_in,
    nrm,
    decay,
    qacc,
    qkvg,
    mixed,
    acts,
    hid,
    own,
    ship1,
    got1,
    sums1,
    over1,
    last1,
    ship2,
    got2,
    sums2,
    over2,
    last2,
    local_sem,
    far_send,
    far_recv,
    far_pair_send,
    far_pair_recv,
    ring_send,
    ring_recv,
    pair_send,
    pair_recv,
    tok_send,
    tok_recv,
    mid_send,
    mid_recv,
    rs1_send,
    rs1_recv,
    rs2_send,
    rs2_recv,
):
    g = lax.axis_index("grp")
    z = lax.axis_index("fs")
    t = lax.axis_index("tp")
    nx = nt // 2
    x, c = lax.div(t, 2), lax.rem(t, 2)
    parity = lax.rem(g, 2)
    twin = {"grp": g + 1 - 2 * parity}
    right, left = {"fs": lax.rem(z + 1, nf)}, {"fs": lax.rem(z + nf - 1, nf)}
    right_far, left_far = {"fs": lax.rem(z + STRIDE, nf)}, {"fs": lax.rem(z + nf - STRIDE, nf)}

    def tp_of(dx, core):
        return lax.rem(x + dx + nx, nx) * 2 + core

    xr, xl, other = {"tp": tp_of(1, c)}, {"tp": tp_of(-1, c)}, {"tp": tp_of(0, 1 - c)}
    far = nf // 2
    rows, width = tok.shape
    half = rows // 2
    per, cols = wq.shape
    ff = wgate.shape[1]
    mcol = 4 * cols
    tiles = width // per

    mine = pl.ds(pl.multiple_of(z * per, per), per)
    copies = [pltpu.make_async_copy(tok, tok_all.at[t], local_sem.at[0])]
    for n, w in enumerate((wq, wk, wv, wo, wm)):
        copies.append(pltpu.make_async_copy(w, a_buf.at[mine, pl.ds(n * cols, cols)], local_sem.at[1 + n]))
    copies.append(pltpu.make_async_copy(wgate, g_buf.at[mine, pl.ds(0, ff)], local_sem.at[6]))
    copies.append(pltpu.make_async_copy(wup, g_buf.at[mine, pl.ds(ff, ff)], local_sem.at[7]))
    copies.append(pltpu.make_async_copy(wdown, d_buf.at[mine, :], local_sem.at[8]))
    for copy in copies:
        copy.start()

    barrier = pltpu.get_barrier_semaphore()
    for peer in (left, right, left_far, right_far, xl, xr, other, twin):
        pl.semaphore_signal(barrier, inc=1, device_id=peer, device_id_type=MESH)
    pl.semaphore_wait(barrier, 8)

    def shared(buf, row0, nrow, col0, ncol, by_row, i, k):
        step_r, step_c = (nrow, 0) if by_row else (0, ncol)
        flip = 1 - parity
        return (buf, row0 + step_r * parity, nrow, col0 + step_c * parity, ncol, i, k, row0 + step_r * flip, col0 + step_c * flip)

    g_common, g_half = 4 * 128, 3 * 128
    d_common, d_half = 128, 2 * 128
    lower = per // 2
    cls_a = shared(a_buf, 0, lower, 0, mcol + wm.shape[1], True, None, None)
    cls_g = shared(g_buf, 0, per, g_common, g_half, False, None, 0)
    cls_d = shared(d_buf, 0, per, d_common, d_half, False, 5, 1)
    cls_g0 = (g_buf, 0, lower, 0, g_common, 0, None, 0, 0)
    cls_g1 = (g_buf, lower, lower, 0, g_common, 1, None, 0, 0)
    cls_g2 = shared(g_buf, 0, lower, g_common, g_half, False, 2, None)
    cls_g3 = shared(g_buf, lower, lower, g_common, g_half, False, 3, None)
    cls_d0 = (d_buf, 0, per, 0, d_common, 4, None, 0, 0)
    paired = {3: cls_g, 5: cls_d}

    def piece(cls, b, twins=False):
        buf, row0, nrow, col0, ncol, _, _, row1, col1 = cls
        r, k = (row1, col1) if twins else (row0, col0)
        r = pl.multiple_of(b * per + r, 16)
        k = k if isinstance(k, int) else pl.multiple_of(k, 128)
        return buf.at[pl.ds(r, nrow), pl.ds(k, ncol)]

    def hop(cls, s, wait_r, wait_l, send_r, send_l):
        i = cls[5]
        for d, (b, source, target, wait, send) in enumerate(
            (
                (lax.rem(z - s + nf, nf), left, right, wait_r, send_r),
                (lax.rem(z + s, nf), right, left, wait_l, send_l),
            )
        ):
            ref = piece(cls, b)
            if wait:
                remote(ref, ref, ring_send.at[i], ring_recv.at[i, d, lax.rem(s, SLOTS)], source).wait_recv()
            if send:
                remote(ref, ref, ring_send.at[i], ring_recv.at[i, d, lax.rem(s + 1, SLOTS)], target).start()
            if wait and i in paired:
                ref, k = piece(paired[i], b), paired[i][6]
                remote(ref, ref, pair_send.at[k], pair_recv.at[k, d, s], twin).start()

    def from_twin(cls, lo, hi):
        k = cls[6]

        def one(s, d):
            b = lax.rem(z - s + nf, nf) if d == 0 else lax.rem(z + s, nf)
            ref = piece(cls, b, True)
            remote(ref, ref, pair_send.at[k], pair_recv.at[k, d, s], twin).wait_recv()

        def body(s, carry):
            one(s, 0)
            one(s, 1)
            return carry

        lax.fori_loop(lo, min(hi, far), body, 0)
        if hi > far:
            one(far, 0)

    stages = (far - 1) // STRIDE

    def at_distance(d, twins=False):
        return piece(cls_a, lax.rem(z - d + nf, nf), twins)

    def pass_on(d, step, device):
        ref = at_distance(d)
        remote(ref, ref, far_send.at[0], far_recv.at[d + step + far - 1], device).start()

    def receive(d):
        ref = at_distance(d)
        remote(ref, ref, far_send.at[0], far_recv.at[d + far - 1], right).wait_recv()

    def to_twin(d):
        ref = at_distance(d)
        remote(ref, ref, far_pair_send.at[0], far_pair_recv.at[d + far - 1], twin).start()

    def twin_blocks(lo, hi):
        for dist in range(lo, hi):
            for d in (dist, -dist) if dist < far else (dist,):
                ref = at_distance(d, True)
                remote(ref, ref, far_pair_send.at[0], far_pair_recv.at[d + far - 1], twin).wait_recv()

    def stage(i):
        for sign, ahead, behind, jump in ((1, right, left, right_far), (-1, left, right, left_far)):
            d = sign * STRIDE * i
            if i > 0:
                receive(d)
            if i < stages:
                pass_on(d, sign * STRIDE, jump)
            if abs(d) + 1 < far or sign > 0:
                pass_on(d, sign, ahead)
            if i > 0:
                pass_on(d, -sign, behind)
                to_twin(d)

    def fills(i):
        near = [1, -1] if i == 0 else [STRIDE * i - 1, 1 - STRIDE * i, STRIDE * i + 1, -STRIDE * i - 1]
        for d in near:
            if d > -far:
                receive(d)
                to_twin(d)

    classes = [(cls_g0, 0), (cls_g1, 0), (cls_g2, 0), (cls_g3, 0), (cls_d0, D_START), (cls_d, D_START)]
    clock = [0]

    def step_kind(s):
        if s < 0 or s > far:
            return None
        if s == 0:
            return (False, False, True, True)
        if s == far - 1:
            return (True, True, True, False)
        if s == far:
            return (True, False, False, False)
        return (True, True, True, True)

    def ticks(n):
        end = min(clock[0] + n, D_START + far + 1)
        while clock[0] < end:
            r = clock[0]
            kinds = [step_kind(r - off) for _, off in classes]
            run = r + 1
            if all(kind is None or kind == (True,) * 4 for kind in kinds):
                while run < end and [step_kind(run - off) for _, off in classes] == kinds:
                    run += 1

                def body(q, carry):
                    for (cls, off), kind in zip(classes, kinds):
                        if kind is not None:
                            hop(cls, q - off, *kind)
                    return carry

                lax.fori_loop(r, run, body, 0)
            else:
                for (cls, off), kind in zip(classes, kinds):
                    if kind is not None:
                        hop(cls, r - off, *kind)
            clock[0] = run

    def put(src, dst, send, recv, i, device):
        remote(src, dst, send.at[0], recv.at[i], device).start()

    def got(dst, send, recv, i, device):
        remote(dst, dst, send.at[0], recv.at[i], device).wait_recv()

    halves = (pl.ds(0, half), pl.ds(half, half))

    def gather_start(buf, send, recv):
        for h in (0, 1):
            part = buf.at[t, halves[h]]
            put(part, part, send, recv, h, xr)
            part = buf.at[t, halves[1 - h]]
            put(part, part, send, recv, 3 - h, xl)
        put(buf.at[t], buf.at[t], send, recv, 6, other)

    def gather_rest(buf, send, recv, pause):
        block_l, block_r, block_o = tp_of(-1, c), tp_of(1, c), tp_of(2, c)
        for i, block, h, source, onward, j in (
            (0, block_l, 0, xl, xr, 4),
            (3, block_r, 1, xr, xl, 5),
            (1, block_l, 1, xl, None, None),
            (2, block_r, 0, xr, None, None),
            (4, block_o, 0, xl, None, None),
            (5, block_o, 1, xr, None, None),
        ):
            if i in (1, 4):
                pause()
            part = buf.at[block, halves[h]]
            got(part, send, recv, i, source)
            if onward is not None:
                put(part, part, send, recv, j, onward)
            put(part, part, send, recv, 7 + i, other)
        pause()
        got(buf.at[tp_of(0, 1 - c)], send, recv, 6, other)
        for i, dx, h in ((0, -1, 0), (1, -1, 1), (2, 1, 0), (3, 1, 1), (4, 2, 0), (5, 2, 1)):
            got(buf.at[tp_of(dx, 1 - c), halves[h]], send, recv, 7 + i, other)

    def reduce_scatter(partial, ship, have, sums, over, last, send, recv, pause):
        def product(r, dx):
            ship[r] = partial(tp_of(dx, 1 - c)).astype(BF16)
            put(ship.at[r], have.at[r], send, recv, r, other)
            own[r] = partial(tp_of(dx, c))

        product(0, 2)
        product(1, 1)
        got(have.at[0], send, recv, 0, other)
        sums[0] = (own[0] + have[0].astype(F32)).astype(BF16)
        put(sums.at[0, halves[0]], over.at[0], send, recv, 4, xr)
        put(sums.at[0, halves[1]], over.at[1], send, recv, 5, xl)
        product(2, -1)
        got(have.at[1], send, recv, 1, other)
        sums[1, halves[1]] = (own[1, halves[1]] + have[1, halves[1]].astype(F32)).astype(BF16)
        put(sums.at[1, halves[1]], last.at[0, halves[1]], send, recv, 6, xr)
        pause()
        product(3, 0)
        got(have.at[2], send, recv, 2, other)
        sums[2, halves[0]] = (own[2, halves[0]] + have[2, halves[0]].astype(F32)).astype(BF16)
        put(sums.at[2, halves[0]], last.at[1, halves[0]], send, recv, 7, xl)
        got(have.at[3], send, recv, 3, other)
        own[3] = own[3] + have[3].astype(F32)
        pause()
        got(over.at[0], send, recv, 4, xl)
        sums[1, halves[0]] = (own[1, halves[0]] + have[1, halves[0]].astype(F32) + over[0].astype(F32)).astype(BF16)
        put(sums.at[1, halves[0]], last.at[0, halves[0]], send, recv, 8, xr)
        got(over.at[1], send, recv, 5, xr)
        sums[2, halves[1]] = (own[2, halves[1]] + have[2, halves[1]].astype(F32) + over[1].astype(F32)).astype(BF16)
        put(sums.at[2, halves[1]], last.at[1, halves[1]], send, recv, 9, xl)
        pause()
        got(last.at[0, halves[1]], send, recv, 6, xl)
        got(last.at[1, halves[0]], send, recv, 7, xr)
        got(last.at[0, halves[0]], send, recv, 8, xl)
        got(last.at[1, halves[1]], send, recv, 9, xr)
        return own[3] + last[0].astype(F32) + last[1].astype(F32)

    def normalize(source, gain, store):
        total = jnp.zeros((rows, 1), F32)
        for j in range(nt):
            v = source[j].astype(F32)
            total = total + jnp.sum(v * v, axis=-1, keepdims=True)
        scale = lax.rsqrt(total * (1.0 / (nt * width)) + NORM_EPS)
        for j in range(nt):
            span = pl.ds(j * width, width)
            store(j, (source[j].astype(F32) * scale * gain[:, span]).astype(BF16))

    first = lax.div(z, tiles)

    def add_group(k, start=False):
        j = lax.rem(first + k + nt, nt)
        rows_j = pl.ds(pl.multiple_of(j * width, width), width)
        term = jnp.dot(nrm_in[j], a_buf[rows_j, pl.ds(0, mcol)], preferred_element_type=F32)
        qacc[...] = term if start else qacc[...] + term

    n_id = lax.broadcasted_iota(jnp.int32, (128, rows), 0)
    m_id = lax.broadcasted_iota(jnp.int32, (128, rows), 1)
    lane = lax.broadcasted_iota(jnp.int32, (rows, 2 * HEAD), 1)
    low_head = lane < HEAD

    def decay_weights(h):
        fwd = jax.nn.log_sigmoid(fdec[...])
        bwd = jax.nn.log_sigmoid(bdec[...])
        for chunk in range(rows // 128):
            gap = (n_id + (chunk * 128) - m_id).astype(F32)
            exponent = jnp.where(gap >= 0, fwd[:, h : h + 1] * gap, bwd[:, h : h + 1] * (-gap))
            decay[h, pl.ds(chunk * 128, 128), :] = jnp.exp(exponent)

    for copy in copies[1:6]:
        copy.wait()
    stage(0)
    copies[0].wait()
    gather_start(tok_all, tok_send, tok_recv)
    for copy in copies[6:]:
        copy.wait()
    ticks(1)
    decay_weights(0)
    stage(1)
    ticks(1)
    fills(0)
    decay_weights(1)
    stage(2)
    ticks(1)
    fills(1)
    gather_rest(tok_all, tok_send, tok_recv, lambda: None)
    stage(3)
    ticks(1)
    fills(2)
    normalize(tok_all, gain1, lambda j, v: nrm_in.__setitem__(j, v))
    ticks(1)
    stage(4)
    ticks(1)
    fills(3)
    twin_blocks(1, 2 * tiles)
    add_group(0, True)
    ticks(1)
    stage(5)
    fills(4)
    add_group(1)
    add_group(-1)
    fills(5)
    ticks(1)
    twin_blocks(2 * tiles, 3 * tiles)
    add_group(2)
    add_group(-2)
    twin_blocks(3 * tiles, far + 1)
    add_group(3)
    add_group(-3)
    add_group(far // tiles)
    qkvg[...] = qacc[...].astype(BF16)
    ticks(1)

    def rotated(n):
        v = qkvg[:, pl.ds(n * cols, cols)].astype(F32)
        lo_half = lax.rem(lane, HEAD) < HEAD // 2
        swapped = jnp.where(lo_half, pltpu.roll(v, 2 * HEAD - HEAD // 2, 1), pltpu.roll(v, HEAD // 2, 1))
        return v * cos[...] + swapped * sin[...]

    rq = rotated(0)
    rk = (rotated(1) * HEAD**-0.5).astype(BF16)
    value = qkvg[:, pl.ds(2 * cols, cols)]
    kept = []
    for h in range(2):
        q_h = jnp.where(low_head if h == 0 else jnp.logical_not(low_head), rq, 0.0).astype(BF16)
        parts = []
        for chunk in range(rows // 128):
            scores = lax.dot_general(q_h[chunk * 128 : (chunk + 1) * 128], rk, NT_DIMS, preferred_element_type=F32)
            weighted = (scores * decay[h, pl.ds(chunk * 128, 128), :]).astype(BF16)
            parts.append(jnp.dot(weighted, value, preferred_element_type=F32))
        kept.append(jnp.concatenate(parts, axis=0))
    retained = jnp.where(low_head, kept[0], kept[1])

    def head_mean(v):
        lo = jnp.sum(jnp.where(low_head, v, 0.0), axis=-1, keepdims=True)
        hi = jnp.sum(jnp.where(low_head, 0.0, v), axis=-1, keepdims=True)
        return jnp.where(low_head, lo, hi) * (1.0 / HEAD)

    centered = retained - head_mean(retained)
    normalized = centered * lax.rsqrt(head_mean(centered * centered) + GROUP_EPS)
    gate = qkvg[:, pl.ds(3 * cols, cols)].astype(F32)
    mixed[...] = (gate / (1.0 + jnp.exp(-gate)) * normalized).astype(BF16)

    def merge_part(j):
        w = a_buf[pl.ds(pl.multiple_of(j * width, width), width), pl.ds(mcol, wm.shape[1])]
        return lax.dot_general(mixed[...], w, NT_DIMS, preferred_element_type=F32)

    merged = reduce_scatter(merge_part, ship1, got1, sums1, over1, last1, rs1_send, rs1_recv, lambda: ticks(1))
    mid_all[t] = (tok_all[t].astype(F32) + merged).astype(BF16)
    gather_start(mid_all, mid_send, mid_recv)
    gather_rest(mid_all, mid_send, mid_recv, lambda: ticks(1))
    normalize(mid_all, gain2, lambda j, v: nrm.__setitem__((slice(None), pl.ds(j * width, width)), v))
    ticks(far + 1 - clock[0])
    from_twin(cls_g, 1, far + 1)
    acts[:, pl.ds(0, ff)] = jnp.dot(nrm[...], g_buf[:, pl.ds(0, ff)], preferred_element_type=F32)
    ticks(1)
    acts[:, pl.ds(ff, ff)] = jnp.dot(nrm[...], g_buf[:, pl.ds(ff, ff)], preferred_element_type=F32)
    ticks(1)
    gated = acts[:, pl.ds(0, ff)]
    hid[...] = (gated / (1.0 + jnp.exp(-gated)) * acts[:, pl.ds(ff, ff)]).astype(BF16)
    ticks(D_START + far + 1)
    from_twin(cls_d, 1, far + 1)

    def down_part(j):
        w = d_buf[pl.ds(pl.multiple_of(j * width, width), width), :]
        return lax.dot_general(hid[...], w, NT_DIMS, preferred_element_type=F32)

    summed = reduce_scatter(down_part, ship2, got2, sums2, over2, last2, rs2_send, rs2_recv, lambda: None)
    out[...] = (mid_all[t].astype(F32) + summed).astype(BF16)

    whole = a_buf.at[pl.ds(0, (nf - 1) * (per // 2)), :]
    remote(whole, whole, far_send.at[0], far_recv.at[0], right).wait_send()
    remote(whole, whole, far_pair_send.at[0], far_pair_recv.at[0], twin).wait_send()
    def drain(cls, sem, recv, device):
        buf, row0, nrow, col0, ncol = cls[:5]
        cut = pl.ds(col0 if isinstance(col0, int) else pl.multiple_of(col0, 128), ncol)
        total = buf.at[pl.ds(0, (nf - 1) * nrow), cut]
        remote(total, total, sem, recv, device).wait_send()

    for cls, _ in classes:
        drain(cls, ring_send.at[cls[5]], ring_recv.at[cls[5], 0, 0], right)
    for cls in paired.values():
        drain(cls, pair_send.at[cls[6]], pair_recv.at[cls[6], 0, 0], twin)
    whole = tok_all.at[pl.ds(0, nt - 1)]
    for sem in (tok_send, mid_send, rs1_send, rs2_send):
        remote(whole, whole, sem.at[0], tok_recv.at[0], other).wait_send()


def on_device(nf, nt, tokens, input_gain, wq, wk, wv, wo, fdec, bdec, wm, middle_gain, wgate, wup, wdown):
    seqs, rows, width = tokens.shape
    per, cols = wq.shape
    ff = wgate.shape[1]
    full = nf * per
    nx = nt // 2
    cos, sin = rotation_tables(rows)
    anywhere = pl.BlockSpec(memory_space=pl.ANY)
    vmem = pl.BlockSpec(memory_space=pltpu.VMEM)
    dma = pltpu.SemaphoreType.DMA
    block = (rows, width)
    exchange = [
        pltpu.VMEM((nx, *block), BF16),
        pltpu.VMEM((nx, *block), BF16),
        pltpu.VMEM((3, *block), BF16),
        pltpu.VMEM((2, rows // 2, width), BF16),
        pltpu.VMEM((2, *block), BF16),
    ]
    out = pl.pallas_call(
        functools.partial(layer_kernel, nf, nt),
        out_shape=jax.ShapeDtypeStruct(block, BF16),
        in_specs=[anywhere, vmem]
        + [anywhere] * 4
        + [vmem, vmem, anywhere, vmem]
        + [anywhere] * 3
        + [vmem, vmem],
        out_specs=vmem,
        scratch_shapes=[
            pltpu.VMEM((full, 4 * cols + wm.shape[0]), BF16),
            pltpu.VMEM((full, 2 * ff), BF16),
            pltpu.VMEM((full, ff), BF16),
            pltpu.VMEM((nt, *block), BF16),
            pltpu.VMEM((nt, *block), BF16),
            pltpu.VMEM((nt, *block), BF16),
            pltpu.VMEM((rows, full), BF16),
            pltpu.VMEM((2, rows, rows), F32),
            pltpu.VMEM((rows, 4 * cols), F32),
            pltpu.VMEM((rows, 4 * cols), BF16),
            pltpu.VMEM((rows, cols), BF16),
            pltpu.VMEM((rows, 2 * ff), F32),
            pltpu.VMEM((rows, ff), BF16),
            pltpu.VMEM((nx, *block), F32),
            *exchange,
            *exchange,
            dma((9,)),
            dma((1,)),
            dma((nf,)),
            dma((1,)),
            dma((nf,)),
            dma((6,)),
            dma((6, 2, SLOTS)),
            dma((2,)),
            dma((2, 2, nf // 2 + 1)),
            dma((1,)),
            dma((13,)),
            dma((1,)),
            dma((13,)),
            dma((1,)),
            dma((10,)),
            dma((1,)),
            dma((10,)),
        ],
        compiler_params=pltpu.CompilerParams(
            collective_id=0, has_side_effects=True, vmem_limit_bytes=60 * 1024 * 1024
        ),
    )(
        tokens.reshape(seqs * rows, width),
        input_gain.reshape(1, -1),
        wq,
        wk,
        wv,
        wo,
        fdec.reshape(1, -1),
        bdec.reshape(1, -1),
        wm.T,
        middle_gain.reshape(1, -1),
        wgate,
        wup,
        wdown.T,
        jnp.asarray(cos),
        jnp.asarray(sin),
    )
    return out.reshape(seqs, rows, width)


def solution(mesh):
    sizes = dict(mesh.shape)
    placed = (
        P(("grp", "fs"), None, "tp"),
        P(),
        P("fs", "tp"),
        P("fs", "tp"),
        P("fs", "tp"),
        P("fs", "tp"),
        P("tp"),
        P("tp"),
        P("tp", "fs"),
        P(),
        P("fs", "tp"),
        P("fs", "tp"),
        P("tp", "fs"),
    )
    return jax.shard_map(
        functools.partial(on_device, sizes["fs"], sizes["tp"]),
        mesh=mesh,
        in_specs=placed,
        out_specs=P(("grp", "fs"), None, "tp"),
        check_vma=False,
    )
```

```python
import functools

import jax
import jax.numpy as jnp
import numpy as np
from jax import lax
from jax.experimental import pallas as pl
from jax.experimental.pallas import tpu as pltpu
from jax.sharding import PartitionSpec as P

MESH = pl.DeviceIdType.MESH
HEAD = 64
NORM_EPS = 1e-06
GROUP_EPS = 1e-05
ROPE_BASE = 10000.0
F32 = jnp.float32
BF16 = jnp.bfloat16

D_START = 0
SLOTS = 4
STRIDE = 3

NT_DIMS = (((1,), (1,)), ((), ()))


def rotation_tables(length):
    half = HEAD // 2
    inverse = ROPE_BASE ** (-np.arange(half, dtype=np.float32) / np.float32(half))
    angles = np.arange(length, dtype=np.float32)[:, None] * inverse.astype(np.float32)[None, :]
    cosine, sine = np.cos(angles), np.sin(angles)
    return (
        np.concatenate([cosine, cosine] * 2, axis=1).astype(np.float32),
        np.concatenate([-sine, sine] * 2, axis=1).astype(np.float32),
    )


def remote(src, dst, send_sem, recv_sem, device):
    return pltpu.make_async_remote_copy(
        src_ref=src, dst_ref=dst, send_sem=send_sem, recv_sem=recv_sem, device_id=device, device_id_type=MESH
    )


def layer_kernel(
    nf,
    nt,
    tok,
    gain1,
    wq,
    wk,
    wv,
    wo,
    fdec,
    bdec,
    wm,
    gain2,
    wgate,
    wup,
    wdown,
    cos,
    sin,
    out,
    a_buf,
    g_buf,
    d_buf,
    tok_all,
    mid_all,
    nrm_in,
    nrm,
    decay,
    qacc,
    qkvg,
    mixed,
    acts,
    hid,
    own,
    ship1,
    got1,
    sums1,
    over1,
    last1,
    ship2,
    got2,
    sums2,
    over2,
    last2,
    local_sem,
    far_send,
    far_recv,
    far_pair_send,
    far_pair_recv,
    ring_send,
    ring_recv,
    pair_send,
    pair_recv,
    tok_send,
    tok_recv,
    mid_send,
    mid_recv,
    rs1_send,
    rs1_recv,
    rs2_send,
    rs2_recv,
):
    g = lax.axis_index("grp")
    z = lax.axis_index("fs")
    t = lax.axis_index("tp")
    nx = nt // 2
    x, c = lax.div(t, 2), lax.rem(t, 2)
    parity = lax.rem(g, 2)
    twin = {"grp": g + 1 - 2 * parity}
    right, left = {"fs": lax.rem(z + 1, nf)}, {"fs": lax.rem(z + nf - 1, nf)}
    right_far, left_far = {"fs": lax.rem(z + STRIDE, nf)}, {"fs": lax.rem(z + nf - STRIDE, nf)}

    def tp_of(dx, core):
        return lax.rem(x + dx + nx, nx) * 2 + core

    xr, xl, other = {"tp": tp_of(1, c)}, {"tp": tp_of(-1, c)}, {"tp": tp_of(0, 1 - c)}
    far = nf // 2
    rows, width = tok.shape
    half = rows // 2
    per, cols = wq.shape
    ff = wgate.shape[1]
    mcol = 4 * cols
    tiles = width // per

    mine = pl.ds(pl.multiple_of(z * per, per), per)
    copies = [pltpu.make_async_copy(tok, tok_all.at[t], local_sem.at[0])]
    for n, w in enumerate((wq, wk, wv, wo, wm)):
        copies.append(pltpu.make_async_copy(w, a_buf.at[mine, pl.ds(n * cols, cols)], local_sem.at[1 + n]))
    copies.append(pltpu.make_async_copy(wgate, g_buf.at[mine, pl.ds(0, ff)], local_sem.at[6]))
    copies.append(pltpu.make_async_copy(wup, g_buf.at[mine, pl.ds(ff, ff)], local_sem.at[7]))
    copies.append(pltpu.make_async_copy(wdown, d_buf.at[mine, :], local_sem.at[8]))
    for copy in copies:
        copy.start()

    barrier = pltpu.get_barrier_semaphore()
    for peer in (left, right, left_far, right_far, xl, xr, other, twin):
        pl.semaphore_signal(barrier, inc=1, device_id=peer, device_id_type=MESH)
    pl.semaphore_wait(barrier, 8)

    def shared(buf, row0, nrow, col0, ncol, by_row, i, k):
        step_r, step_c = (nrow, 0) if by_row else (0, ncol)
        flip = 1 - parity
        return (buf, row0 + step_r * parity, nrow, col0 + step_c * parity, ncol, i, k, row0 + step_r * flip, col0 + step_c * flip)

    g_common, g_half = 4 * 128, 3 * 128
    d_common, d_half = 128, 2 * 128
    lower = per // 2
    cls_a = shared(a_buf, 0, lower, 0, mcol + wm.shape[1], True, None, None)
    cls_g = shared(g_buf, 0, per, g_common, g_half, False, None, 0)
    cls_d = shared(d_buf, 0, per, d_common, d_half, False, 5, 1)
    cls_g0 = (g_buf, 0, lower, 0, g_common, 0, None, 0, 0)
    cls_g1 = (g_buf, lower, lower, 0, g_common, 1, None, 0, 0)
    cls_g2 = shared(g_buf, 0, lower, g_common, g_half, False, 2, None)
    cls_g3 = shared(g_buf, lower, lower, g_common, g_half, False, 3, None)
    cls_d0 = (d_buf, 0, per, 0, d_common, 4, None, 0, 0)
    paired = {3: cls_g, 5: cls_d}

    def piece(cls, b, twins=False):
        buf, row0, nrow, col0, ncol, _, _, row1, col1 = cls
        r, k = (row1, col1) if twins else (row0, col0)
        r = pl.multiple_of(b * per + r, 16)
        k = k if isinstance(k, int) else pl.multiple_of(k, 128)
        return buf.at[pl.ds(r, nrow), pl.ds(k, ncol)]

    def hop(cls, s, wait_r, wait_l, send_r, send_l):
        i = cls[5]
        for d, (b, source, target, wait, send) in enumerate(
            (
                (lax.rem(z - s + nf, nf), left, right, wait_r, send_r),
                (lax.rem(z + s, nf), right, left, wait_l, send_l),
            )
        ):
            ref = piece(cls, b)
            if wait:
                remote(ref, ref, ring_send.at[i], ring_recv.at[i, d, lax.rem(s, SLOTS)], source).wait_recv()
            if send:
                remote(ref, ref, ring_send.at[i], ring_recv.at[i, d, lax.rem(s + 1, SLOTS)], target).start()
            if wait and i in paired:
                ref, k = piece(paired[i], b), paired[i][6]
                remote(ref, ref, pair_send.at[k], pair_recv.at[k, d, s], twin).start()

    def from_twin(cls, lo, hi):
        k = cls[6]

        def one(s, d):
            b = lax.rem(z - s + nf, nf) if d == 0 else lax.rem(z + s, nf)
            ref = piece(cls, b, True)
            remote(ref, ref, pair_send.at[k], pair_recv.at[k, d, s], twin).wait_recv()

        def body(s, carry):
            one(s, 0)
            one(s, 1)
            return carry

        lax.fori_loop(lo, min(hi, far), body, 0)
        if hi > far:
            one(far, 0)

    stages = (far - 1) // STRIDE

    def at_distance(d, twins=False):
        return piece(cls_a, lax.rem(z - d + nf, nf), twins)

    def pass_on(d, step, device):
        ref = at_distance(d)
        remote(ref, ref, far_send.at[0], far_recv.at[d + step + far - 1], device).start()

    def receive(d):
        ref = at_distance(d)
        remote(ref, ref, far_send.at[0], far_recv.at[d + far - 1], right).wait_recv()

    def to_twin(d):
        ref = at_distance(d)
        remote(ref, ref, far_pair_send.at[0], far_pair_recv.at[d + far - 1], twin).start()

    def twin_blocks(lo, hi):
        for dist in range(lo, hi):
            for d in (dist, -dist) if dist < far else (dist,):
                ref = at_distance(d, True)
                remote(ref, ref, far_pair_send.at[0], far_pair_recv.at[d + far - 1], twin).wait_recv()

    def stage(i):
        for sign, ahead, behind, jump in ((1, right, left, right_far), (-1, left, right, left_far)):
            d = sign * STRIDE * i
            if i > 0:
                receive(d)
            if i < stages:
                pass_on(d, sign * STRIDE, jump)
            if abs(d) + 1 < far or sign > 0:
                pass_on(d, sign, ahead)
            if i > 0:
                pass_on(d, -sign, behind)
                to_twin(d)

    def fills(i):
        near = [1, -1] if i == 0 else [STRIDE * i - 1, 1 - STRIDE * i, STRIDE * i + 1, -STRIDE * i - 1]
        for d in near:
            if d > -far:
                receive(d)
                to_twin(d)

    classes = [(cls_d0, D_START), (cls_g2, 0), (cls_g3, 0), (cls_g0, 0), (cls_g1, 0), (cls_d, D_START)]
    clock = [0]

    def step_kind(s):
        if s < 0 or s > far:
            return None
        if s == 0:
            return (False, False, True, True)
        if s == far - 1:
            return (True, True, True, False)
        if s == far:
            return (True, False, False, False)
        return (True, True, True, True)

    def ticks(n):
        end = min(clock[0] + n, D_START + far + 1)
        while clock[0] < end:
            r = clock[0]
            kinds = [step_kind(r - off) for _, off in classes]
            run = r + 1
            if all(kind is None or kind == (True,) * 4 for kind in kinds):
                while run < end and [step_kind(run - off) for _, off in classes] == kinds:
                    run += 1

                def body(q, carry):
                    for (cls, off), kind in zip(classes, kinds):
                        if kind is not None:
                            hop(cls, q - off, *kind)
                    return carry

                lax.fori_loop(r, run, body, 0)
            else:
                for (cls, off), kind in zip(classes, kinds):
                    if kind is not None:
                        hop(cls, r - off, *kind)
            clock[0] = run

    def put(src, dst, send, recv, i, device):
        remote(src, dst, send.at[0], recv.at[i], device).start()

    def got(dst, send, recv, i, device):
        remote(dst, dst, send.at[0], recv.at[i], device).wait_recv()

    halves = (pl.ds(0, half), pl.ds(half, half))

    def gather_start(buf, send, recv):
        for h in (0, 1):
            part = buf.at[t, halves[h]]
            put(part, part, send, recv, h, xr)
            part = buf.at[t, halves[1 - h]]
            put(part, part, send, recv, 3 - h, xl)
        put(buf.at[t], buf.at[t], send, recv, 6, other)

    def gather_rest(buf, send, recv, pause):
        block_l, block_r, block_o = tp_of(-1, c), tp_of(1, c), tp_of(2, c)
        for i, block, h, source, onward, j in (
            (0, block_l, 0, xl, xr, 4),
            (3, block_r, 1, xr, xl, 5),
            (1, block_l, 1, xl, None, None),
            (2, block_r, 0, xr, None, None),
            (4, block_o, 0, xl, None, None),
            (5, block_o, 1, xr, None, None),
        ):
            if i in (1, 4):
                pause()
            part = buf.at[block, halves[h]]
            got(part, send, recv, i, source)
            if onward is not None:
                put(part, part, send, recv, j, onward)
            put(part, part, send, recv, 7 + i, other)
        pause()
        got(buf.at[tp_of(0, 1 - c)], send, recv, 6, other)
        for i, dx, h in ((0, -1, 0), (1, -1, 1), (2, 1, 0), (3, 1, 1), (4, 2, 0), (5, 2, 1)):
            got(buf.at[tp_of(dx, 1 - c), halves[h]], send, recv, 7 + i, other)

    def reduce_scatter(partial, ship, have, sums, over, last, send, recv, pause):
        def product(r, dx):
            ship[r] = partial(tp_of(dx, 1 - c)).astype(BF16)
            put(ship.at[r], have.at[r], send, recv, r, other)
            own[r] = partial(tp_of(dx, c))

        product(0, 2)
        product(1, 1)
        got(have.at[0], send, recv, 0, other)
        sums[0] = (own[0] + have[0].astype(F32)).astype(BF16)
        put(sums.at[0, halves[0]], over.at[0], send, recv, 4, xr)
        put(sums.at[0, halves[1]], over.at[1], send, recv, 5, xl)
        product(2, -1)
        got(have.at[1], send, recv, 1, other)
        sums[1, halves[1]] = (own[1, halves[1]] + have[1, halves[1]].astype(F32)).astype(BF16)
        put(sums.at[1, halves[1]], last.at[0, halves[1]], send, recv, 6, xr)
        pause()
        product(3, 0)
        got(have.at[2], send, recv, 2, other)
        sums[2, halves[0]] = (own[2, halves[0]] + have[2, halves[0]].astype(F32)).astype(BF16)
        put(sums.at[2, halves[0]], last.at[1, halves[0]], send, recv, 7, xl)
        got(have.at[3], send, recv, 3, other)
        own[3] = own[3] + have[3].astype(F32)
        pause()
        got(over.at[0], send, recv, 4, xl)
        sums[1, halves[0]] = (own[1, halves[0]] + have[1, halves[0]].astype(F32) + over[0].astype(F32)).astype(BF16)
        put(sums.at[1, halves[0]], last.at[0, halves[0]], send, recv, 8, xr)
        got(over.at[1], send, recv, 5, xr)
        sums[2, halves[1]] = (own[2, halves[1]] + have[2, halves[1]].astype(F32) + over[1].astype(F32)).astype(BF16)
        put(sums.at[2, halves[1]], last.at[1, halves[1]], send, recv, 9, xl)
        pause()
        got(last.at[0, halves[1]], send, recv, 6, xl)
        got(last.at[1, halves[0]], send, recv, 7, xr)
        got(last.at[0, halves[0]], send, recv, 8, xl)
        got(last.at[1, halves[1]], send, recv, 9, xr)
        return own[3] + last[0].astype(F32) + last[1].astype(F32)

    def normalize(source, gain, store):
        total = jnp.zeros((rows, 1), F32)
        for j in range(nt):
            v = source[j].astype(F32)
            total = total + jnp.sum(v * v, axis=-1, keepdims=True)
        scale = lax.rsqrt(total * (1.0 / (nt * width)) + NORM_EPS)
        for j in range(nt):
            span = pl.ds(j * width, width)
            store(j, (source[j].astype(F32) * scale * gain[:, span]).astype(BF16))

    first = lax.div(z, tiles)

    def add_group(k, start=False):
        j = lax.rem(first + k + nt, nt)
        rows_j = pl.ds(pl.multiple_of(j * width, width), width)
        term = jnp.dot(nrm_in[j], a_buf[rows_j, pl.ds(0, mcol)], preferred_element_type=F32)
        qacc[...] = term if start else qacc[...] + term

    n_id = lax.broadcasted_iota(jnp.int32, (128, rows), 0)
    m_id = lax.broadcasted_iota(jnp.int32, (128, rows), 1)
    lane = lax.broadcasted_iota(jnp.int32, (rows, 2 * HEAD), 1)
    low_head = lane < HEAD

    def decay_weights(h):
        fwd = jax.nn.log_sigmoid(fdec[...])
        bwd = jax.nn.log_sigmoid(bdec[...])
        for chunk in range(rows // 128):
            gap = (n_id + (chunk * 128) - m_id).astype(F32)
            exponent = jnp.where(gap >= 0, fwd[:, h : h + 1] * gap, bwd[:, h : h + 1] * (-gap))
            decay[h, pl.ds(chunk * 128, 128), :] = jnp.exp(exponent)

    for copy in copies[1:6]:
        copy.wait()
    stage(0)
    copies[0].wait()
    gather_start(tok_all, tok_send, tok_recv)
    for copy in copies[6:]:
        copy.wait()
    ticks(1)
    decay_weights(0)
    stage(1)
    ticks(1)
    fills(0)
    decay_weights(1)
    stage(2)
    ticks(1)
    fills(1)
    gather_rest(tok_all, tok_send, tok_recv, lambda: None)
    stage(3)
    ticks(1)
    fills(2)
    normalize(tok_all, gain1, lambda j, v: nrm_in.__setitem__(j, v))
    ticks(1)
    stage(4)
    ticks(1)
    fills(3)
    twin_blocks(1, 2 * tiles)
    add_group(0, True)
    ticks(1)
    stage(5)
    fills(4)
    add_group(1)
    add_group(-1)
    fills(5)
    ticks(1)
    twin_blocks(2 * tiles, 3 * tiles)
    add_group(2)
    add_group(-2)
    twin_blocks(3 * tiles, far + 1)
    add_group(3)
    add_group(-3)
    add_group(far // tiles)
    qkvg[...] = qacc[...].astype(BF16)
    ticks(1)

    def rotated(n):
        v = qkvg[:, pl.ds(n * cols, cols)].astype(F32)
        lo_half = lax.rem(lane, HEAD) < HEAD // 2
        swapped = jnp.where(lo_half, pltpu.roll(v, 2 * HEAD - HEAD // 2, 1), pltpu.roll(v, HEAD // 2, 1))
        return v * cos[...] + swapped * sin[...]

    rq = rotated(0)
    rk = (rotated(1) * HEAD**-0.5).astype(BF16)
    value = qkvg[:, pl.ds(2 * cols, cols)]
    kept = []
    for h in range(2):
        q_h = jnp.where(low_head if h == 0 else jnp.logical_not(low_head), rq, 0.0).astype(BF16)
        parts = []
        for chunk in range(rows // 128):
            scores = lax.dot_general(q_h[chunk * 128 : (chunk + 1) * 128], rk, NT_DIMS, preferred_element_type=F32)
            weighted = (scores * decay[h, pl.ds(chunk * 128, 128), :]).astype(BF16)
            parts.append(jnp.dot(weighted, value, preferred_element_type=F32))
        kept.append(jnp.concatenate(parts, axis=0))
    retained = jnp.where(low_head, kept[0], kept[1])

    def head_mean(v):
        lo = jnp.sum(jnp.where(low_head, v, 0.0), axis=-1, keepdims=True)
        hi = jnp.sum(jnp.where(low_head, 0.0, v), axis=-1, keepdims=True)
        return jnp.where(low_head, lo, hi) * (1.0 / HEAD)

    centered = retained - head_mean(retained)
    normalized = centered * lax.rsqrt(head_mean(centered * centered) + GROUP_EPS)
    gate = qkvg[:, pl.ds(3 * cols, cols)].astype(F32)
    mixed[...] = (gate / (1.0 + jnp.exp(-gate)) * normalized).astype(BF16)

    def merge_part(j):
        w = a_buf[pl.ds(pl.multiple_of(j * width, width), width), pl.ds(mcol, wm.shape[1])]
        return lax.dot_general(mixed[...], w, NT_DIMS, preferred_element_type=F32)

    merged = reduce_scatter(merge_part, ship1, got1, sums1, over1, last1, rs1_send, rs1_recv, lambda: ticks(1))
    mid_all[t] = (tok_all[t].astype(F32) + merged).astype(BF16)
    gather_start(mid_all, mid_send, mid_recv)
    gather_rest(mid_all, mid_send, mid_recv, lambda: ticks(1))
    normalize(mid_all, gain2, lambda j, v: nrm.__setitem__((slice(None), pl.ds(j * width, width)), v))
    ticks(far + 1 - clock[0])
    from_twin(cls_g, 1, far + 1)
    acts[:, pl.ds(0, ff)] = jnp.dot(nrm[...], g_buf[:, pl.ds(0, ff)], preferred_element_type=F32)
    ticks(1)
    acts[:, pl.ds(ff, ff)] = jnp.dot(nrm[...], g_buf[:, pl.ds(ff, ff)], preferred_element_type=F32)
    ticks(1)
    gated = acts[:, pl.ds(0, ff)]
    hid[...] = (gated / (1.0 + jnp.exp(-gated)) * acts[:, pl.ds(ff, ff)]).astype(BF16)
    ticks(D_START + far + 1)
    from_twin(cls_d, 1, far + 1)

    def down_part(j):
        w = d_buf[pl.ds(pl.multiple_of(j * width, width), width), :]
        return lax.dot_general(hid[...], w, NT_DIMS, preferred_element_type=F32)

    summed = reduce_scatter(down_part, ship2, got2, sums2, over2, last2, rs2_send, rs2_recv, lambda: None)
    out[...] = (mid_all[t].astype(F32) + summed).astype(BF16)

    whole = a_buf.at[pl.ds(0, (nf - 1) * (per // 2)), :]
    remote(whole, whole, far_send.at[0], far_recv.at[0], right).wait_send()
    remote(whole, whole, far_pair_send.at[0], far_pair_recv.at[0], twin).wait_send()
    def drain(cls, sem, recv, device):
        buf, row0, nrow, col0, ncol = cls[:5]
        cut = pl.ds(col0 if isinstance(col0, int) else pl.multiple_of(col0, 128), ncol)
        total = buf.at[pl.ds(0, (nf - 1) * nrow), cut]
        remote(total, total, sem, recv, device).wait_send()

    for cls, _ in classes:
        drain(cls, ring_send.at[cls[5]], ring_recv.at[cls[5], 0, 0], right)
    for cls in paired.values():
        drain(cls, pair_send.at[cls[6]], pair_recv.at[cls[6], 0, 0], twin)
    whole = tok_all.at[pl.ds(0, nt - 1)]
    for sem in (tok_send, mid_send, rs1_send, rs2_send):
        remote(whole, whole, sem.at[0], tok_recv.at[0], other).wait_send()


def on_device(nf, nt, tokens, input_gain, wq, wk, wv, wo, fdec, bdec, wm, middle_gain, wgate, wup, wdown):
    seqs, rows, width = tokens.shape
    per, cols = wq.shape
    ff = wgate.shape[1]
    full = nf * per
    nx = nt // 2
    cos, sin = rotation_tables(rows)
    anywhere = pl.BlockSpec(memory_space=pl.ANY)
    vmem = pl.BlockSpec(memory_space=pltpu.VMEM)
    dma = pltpu.SemaphoreType.DMA
    block = (rows, width)
    exchange = [
        pltpu.VMEM((nx, *block), BF16),
        pltpu.VMEM((nx, *block), BF16),
        pltpu.VMEM((3, *block), BF16),
        pltpu.VMEM((2, rows // 2, width), BF16),
        pltpu.VMEM((2, *block), BF16),
    ]
    out = pl.pallas_call(
        functools.partial(layer_kernel, nf, nt),
        out_shape=jax.ShapeDtypeStruct(block, BF16),
        in_specs=[anywhere, vmem]
        + [anywhere] * 4
        + [vmem, vmem, anywhere, vmem]
        + [anywhere] * 3
        + [vmem, vmem],
        out_specs=vmem,
        scratch_shapes=[
            pltpu.VMEM((full, 4 * cols + wm.shape[0]), BF16),
            pltpu.VMEM((full, 2 * ff), BF16),
            pltpu.VMEM((full, ff), BF16),
            pltpu.VMEM((nt, *block), BF16),
            pltpu.VMEM((nt, *block), BF16),
            pltpu.VMEM((nt, *block), BF16),
            pltpu.VMEM((rows, full), BF16),
            pltpu.VMEM((2, rows, rows), F32),
            pltpu.VMEM((rows, 4 * cols), F32),
            pltpu.VMEM((rows, 4 * cols), BF16),
            pltpu.VMEM((rows, cols), BF16),
            pltpu.VMEM((rows, 2 * ff), F32),
            pltpu.VMEM((rows, ff), BF16),
            pltpu.VMEM((nx, *block), F32),
            *exchange,
            *exchange,
            dma((9,)),
            dma((1,)),
            dma((nf,)),
            dma((1,)),
            dma((nf,)),
            dma((6,)),
            dma((6, 2, SLOTS)),
            dma((2,)),
            dma((2, 2, nf // 2 + 1)),
            dma((1,)),
            dma((13,)),
            dma((1,)),
            dma((13,)),
            dma((1,)),
            dma((10,)),
            dma((1,)),
            dma((10,)),
        ],
        compiler_params=pltpu.CompilerParams(
            collective_id=0, has_side_effects=True, vmem_limit_bytes=60 * 1024 * 1024
        ),
    )(
        tokens.reshape(seqs * rows, width),
        input_gain.reshape(1, -1),
        wq,
        wk,
        wv,
        wo,
        fdec.reshape(1, -1),
        bdec.reshape(1, -1),
        wm.T,
        middle_gain.reshape(1, -1),
        wgate,
        wup,
        wdown.T,
        jnp.asarray(cos),
        jnp.asarray(sin),
    )
    return out.reshape(seqs, rows, width)


def solution(mesh):
    sizes = dict(mesh.shape)
    placed = (
        P(("grp", "fs"), None, "tp"),
        P(),
        P("fs", "tp"),
        P("fs", "tp"),
        P("fs", "tp"),
        P("fs", "tp"),
        P("tp"),
        P("tp"),
        P("tp", "fs"),
        P(),
        P("fs", "tp"),
        P("fs", "tp"),
        P("tp", "fs"),
    )
    return jax.shard_map(
        functools.partial(on_device, sizes["fs"], sizes["tp"]),
        mesh=mesh,
        in_specs=placed,
        out_specs=P(("grp", "fs"), None, "tp"),
        check_vma=False,
    )
```
